32 devices in a mesh: sp: 8 (over z, x), tp: 4 (over y, core).
Axes of the slice: x: 2, y: 2, z: 4, core: 2. Of those that a mesh axis runs over, the one named last changes fastest.
Arguments:
- tokens: bfloat16 [8192, 2048], P('sp', 'tp'), may hold values from -16 to 16
- norm_gain: float32 [2048], replicated, may hold values from 0.1 to 1.9
- signal_proj: bfloat16 [2048, 1024], P(None, 'tp'), may hold values from -0.125 to 0.125
- postgate_proj: bfloat16 [2048, 1024], P(None, 'tp'), may hold values from -0.125 to 0.125
- pregate_proj: bfloat16 [2048, 1024], P(None, 'tp'), may hold values from -0.125 to 0.125
- query_proj: bfloat16 [2048, 1024], P(None, 'tp'), may hold values from -0.21875 to 0.21875
- key_proj: bfloat16 [2048, 1024], P(None, 'tp'), may hold values from -0.21875 to 0.21875
- value_proj: bfloat16 [2048, 1024], P(None, 'tp'), may hold values from -0.125 to 0.125
- filter_taps: bfloat16 [3, 1024], P(None, 'tp'), may hold values from -3.5 to 3.5
- break_bias: bfloat16 [8192, 16], P('sp', 'tp'), may hold values from -18 to 0
- filter_readout: bfloat16 [1024, 2048], replicated, may hold values from -0.125 to 0.125
- attention_readout: bfloat16 [1024, 2048], replicated, may hold values from -0.125 to 0.125
Outputs:
- mixed: bfloat16 [8192, 2048], P(('sp', 'tp'))
- mass_logarithm: float32 [16, 8192], P('tp', 'sp')
The draws below stay inside these ranges and needn't reach their ends.
All inputs are finite; a program needn't handle non-finite values.
Results may differ from the reference program's by a relative error of at most 0.013.
Values may be sent and summed in bfloat16 or wider, within the bound.
A program may use at most 128 MiB of HBM per device.

```python
import math
import jax
import jax.numpy as jnp
from jax import lax

D = 2048
CONV_WIDTH = 1024
HEAD_COUNT = 16
HEAD_DIM = 64
CONV_W = 3
TOK_DEV = 1024
ATT_WIDTH = 1024
TOKEN_COUNT = 8192
N_SP = 8


def draw_tokens(key, part):
    row_scale = jnp.exp(jax.random.uniform(jax.random.fold_in(key, 11), (TOKEN_COUNT, 1), jnp.float32, math.log(0.3), math.log(3.0)))
    col_scale = jnp.exp(jnp.linspace(math.log(0.4), math.log(2.5), D) + jax.random.uniform(jax.random.fold_in(key, 12), (D,), jnp.float32, -0.4, 0.4))
    base = jax.random.normal(jax.random.fold_in(key, 13), (TOKEN_COUNT, D), jnp.float32)
    value_matrix = jnp.clip(base * row_scale * col_scale[None, :], -16.0, 16.0)
    return value_matrix.astype(jnp.bfloat16)


def draw_break_bias(key, part):
    head_rank = jax.random.permutation(jax.random.fold_in(key, 21), HEAD_COUNT)
    slow_heads = head_rank < HEAD_COUNT // 2
    slow_rate = jax.random.uniform(jax.random.fold_in(key, 22), (HEAD_COUNT,), jnp.float32, 0.25, 1.0) / TOKEN_COUNT
    span_low = max(2.0, min(30.0, TOK_DEV / 8.0))
    span_high = max(4.0, min(100.0, TOK_DEV / 3.0))
    fast_span = jax.random.uniform(jax.random.fold_in(key, 23), (HEAD_COUNT,), jnp.float32, span_low, span_high)
    break_rate = jnp.where(slow_heads, slow_rate, 1.0 / fast_span)
    block_count = TOKEN_COUNT // TOK_DEV
    block_factor = jax.random.uniform(jax.random.fold_in(key, 24), (block_count, HEAD_COUNT), jnp.float32, -0.7, 0.7)
    blockwise = jnp.repeat(block_factor, TOK_DEV, axis=0)
    rough = jax.random.uniform(jax.random.fold_in(key, 25), (TOKEN_COUNT, HEAD_COUNT), jnp.float32, -0.5, 0.5)
    value_matrix = jnp.log(break_rate)[None, :] - 4.5 + blockwise + rough
    spike_places = jax.random.randint(jax.random.fold_in(key, 26), (4,), 0, TOKEN_COUNT)
    spike_found = jnp.any(jnp.arange(TOKEN_COUNT)[:, None] == spike_places[None, :], axis=1)
    spike_value = jax.random.uniform(jax.random.fold_in(key, 27), (TOKEN_COUNT, HEAD_COUNT), jnp.float32, -1.5, 0.0)
    value_matrix = jnp.where(spike_found[:, None], spike_value, value_matrix)
    value_matrix = jnp.clip(value_matrix, -18.0, 0.0)
    return value_matrix.astype(jnp.bfloat16)


def shard_levels(key, shape, pieces, low, largest):
    level, own = 1.0, jax.random.fold_in(key, 6)
    for dim, shards_of in pieces:
        heights = jnp.exp(jax.random.uniform(jax.random.fold_in(own, dim), (shards_of,), jnp.float32, low / len(pieces), largest / len(pieces)))
        level = level * jnp.repeat(heights, shape[dim] // shards_of).reshape([-1 if axis == dim else 1 for axis in range(len(shape))])
    return level


def gaussian(own_key, extent, width, limit, shards=(), kind=jnp.bfloat16):
    factor_of = shard_levels(own_key, extent, shards, -0.22, 0.18) if shards else 1.0
    values = jax.random.normal(own_key, extent, jnp.float32) * width * factor_of
    return jnp.minimum(jnp.maximum(values, -limit), limit).astype(kind)


def setup_inputs(seed: int = 0) -> dict:
    key_list = jax.random.split(jax.random.key(seed), 13)
    return {
        "tokens": draw_tokens(jax.random.fold_in(key_list[12], 71), 0),
        "norm_gain": jnp.clip(1.0 + 0.18 * jax.random.normal(key_list[1], (D,), jnp.float32), 0.1, 1.9),
        "signal_proj": gaussian(key_list[2], (D, CONV_WIDTH), D ** -0.5, 0.125, ((1, 4),)),
        "postgate_proj": gaussian(key_list[3], (D, CONV_WIDTH), D ** -0.5, 0.125, ((1, 4),)),
        "pregate_proj": gaussian(key_list[4], (D, CONV_WIDTH), D ** -0.5, 0.125, ((1, 4),)),
        "query_proj": gaussian(key_list[5], (D, ATT_WIDTH), (D // 3) ** -0.5, 0.21875, ((1, 4),)),
        "key_proj": gaussian(key_list[6], (D, ATT_WIDTH), (D // 3) ** -0.5, 0.21875, ((1, 4),)),
        "value_proj": gaussian(key_list[7], (D, ATT_WIDTH), D ** -0.5, 0.125, ((1, 4),)),
        "filter_taps": gaussian(key_list[8], (CONV_W, CONV_WIDTH), CONV_W ** -0.5, 3.5, ((1, 4),)),
        "break_bias": draw_break_bias(jax.random.fold_in(key_list[12], 71), 0),
        "filter_readout": gaussian(key_list[10], (CONV_WIDTH, D), (CONV_WIDTH + ATT_WIDTH) ** -0.5, 0.125),
        "attention_readout": gaussian(key_list[11], (ATT_WIDTH, D), (CONV_WIDTH + ATT_WIDTH) ** -0.5, 0.125),
    }


epsilon = 1e-06
mass_floor = 0.1

def project(scaled, weight, inverse):
    product = jnp.dot(scaled, weight, preferred_element_type=jnp.float32)
    return (product * inverse[:, None]).astype(jnp.bfloat16)

def filter_mix(signal, post_gate, pre_gate, filter_taps):
    product = pre_gate.astype(jnp.float32) * signal.astype(jnp.float32)
    padded = jnp.concatenate([jnp.zeros((CONV_W - 1, product.shape[1]), jnp.float32), product], axis=0)
    length = product.shape[0]
    tap_values = filter_taps.astype(jnp.float32)
    running = jnp.zeros_like(product)
    for offset in range(CONV_W):
        running = running + tap_values[offset][None, :] * padded[offset:offset + length]
    return (post_gate.astype(jnp.float32) * running).astype(jnp.bfloat16)

def head_attention(operands):
    queries, key_rows, value_rows, bias_row = operands
    outputs = []
    remains = []
    score_scale = HEAD_DIM ** (-0.5)
    for segment in range(N_SP):
        prefix_blocks = segment + 1
        query_block = queries[segment * TOK_DEV:(segment + 1) * TOK_DEV].astype(jnp.float32)
        key_blocks = key_rows[:prefix_blocks * TOK_DEV].astype(jnp.float32).reshape(prefix_blocks, TOK_DEV, HEAD_DIM)
        value_blocks = value_rows[:prefix_blocks * TOK_DEV].astype(jnp.float32).reshape(prefix_blocks, TOK_DEV, HEAD_DIM)
        bias_blocks = bias_row[:prefix_blocks * TOK_DEV].reshape(prefix_blocks, TOK_DEV)
        scores = jnp.einsum('td,nsd->nts', query_block, key_blocks) * score_scale + bias_blocks[:, None, :]
        block_ids = jnp.arange(prefix_blocks)[:, None, None]
        row_ids = jnp.arange(TOK_DEV)[None, :, None]
        col_ids = jnp.arange(TOK_DEV)[None, None, :]
        allowed = (block_ids < segment) | (col_ids < row_ids)
        log_remainder = jnp.where(allowed, jax.nn.log_sigmoid(-scores), 0.0)
        running = jnp.cumsum(log_remainder, axis=2)
        block_total = running[:, :, -1:]
        later_sum = block_total - running
        weights = jnp.where(allowed, jnp.exp(jax.nn.log_sigmoid(scores) + later_sum), 0.0).astype(jnp.bfloat16)
        partial_value = jnp.einsum('nts,nsd->ntd', weights.astype(jnp.float32), value_blocks)
        totals = block_total[:, :, 0]
        carried = lax.optimization_barrier(jnp.sum(totals, axis=0))[None, :] - jnp.cumsum(totals, axis=0)
        outputs.append(lax.optimization_barrier(jnp.sum(partial_value * jnp.exp(carried)[:, :, None], axis=0)))
        remains.append(lax.optimization_barrier(jnp.sum(totals, axis=0)))
    return (jnp.concatenate(outputs, axis=0), jnp.concatenate(remains, axis=0))

def reference(tokens, norm_gain, signal_proj, postgate_proj, pregate_proj, query_proj, key_proj, value_proj, filter_taps, break_bias, filter_readout, attention_readout):
    widened = tokens.astype(jnp.float32)
    inverse = lax.rsqrt(lax.optimization_barrier(jnp.mean(widened * widened, axis=1)) + epsilon)
    scaled = (widened * norm_gain.astype(jnp.float32)[None, :]).astype(jnp.bfloat16)
    signal = project(scaled, signal_proj, inverse)
    post_gate = project(scaled, postgate_proj, inverse)
    pre_gate = project(scaled, pregate_proj, inverse)
    queries = project(scaled, query_proj, inverse)
    key_rows = project(scaled, key_proj, inverse)
    value_rows = project(scaled, value_proj, inverse)
    filtered = filter_mix(signal, post_gate, pre_gate, filter_taps)
    query_heads = queries.reshape(TOKEN_COUNT, HEAD_COUNT, HEAD_DIM).transpose(1, 0, 2)
    key_heads = key_rows.reshape(TOKEN_COUNT, HEAD_COUNT, HEAD_DIM).transpose(1, 0, 2)
    value_heads = value_rows.reshape(TOKEN_COUNT, HEAD_COUNT, HEAD_DIM).transpose(1, 0, 2)
    bias_heads = break_bias.astype(jnp.float32).T
    head_out, head_remain = lax.map(head_attention, (query_heads, key_heads, value_heads, bias_heads))
    attended = head_out.transpose(1, 0, 2).reshape(TOKEN_COUNT, HEAD_COUNT * HEAD_DIM).astype(jnp.bfloat16)
    mass_logarithm = jnp.log(jnp.maximum(-jnp.expm1(head_remain), mass_floor))
    mixed = (jnp.dot(filtered, filter_readout, preferred_element_type=jnp.float32) + jnp.dot(attended, attention_readout, preferred_element_type=jnp.float32)).astype(jnp.bfloat16)
    return (mixed, mass_logarithm)
```

```python
import functools

import jax
import jax.numpy as jnp
from jax import lax
from jax.experimental import pallas as pl
from jax.experimental.pallas import tpu as pltpu
from jax.sharding import PartitionSpec as P

HEAD_DIM = 64
CONV_W = 3
KEY_CHUNK = 256


epsilon = 1e-06
mass_floor = 0.1
score_cap = 88.0
score_cap_fast = 43.0


def passed_along(block, axis, distance):
    devices = range(lax.axis_size(axis))
    route = [(i - distance, i) for i in devices if i - distance in devices]
    return lax.ppermute(block, axis, route)


def attention_kernel(tok_dev, share, rows, chain, part_ref, recv_ref, bias_ref, out_ref, acc, carry):
    chunk = KEY_CHUNK
    tile = pl.program_id(0)
    tiles_block = share // rows
    block = tile // tiles_block
    inner = (tile % tiles_block) * rows
    row_start = block * tok_dev + part_ref[0] * share + inner
    chunks_block = tok_dev // chunk
    acc[...] = jnp.zeros_like(acc)
    carry[...] = jnp.zeros_like(carry)
    later = lax.broadcasted_iota(jnp.int32, (chunk, chunk), 0)
    earlier = lax.broadcasted_iota(jnp.int32, (chunk, chunk), 1)
    after = jnp.where(later > earlier, 1.0, 0.0).astype(jnp.bfloat16)

    def step(masked, index):
        offset = pl.multiple_of((index % chunks_block) * chunk, chunk)
        key_value = recv_ref[index // chunks_block, pl.ds(offset, chunk), :]
        bias = bias_ref[index]
        for link in range(rows // chain):
            place = pl.ds(link * chain, chain)
            query_place = pl.multiple_of(tok_dev + inner + link * chain, chain)
            query = recv_ref[block, pl.ds(query_place, chain), :]
            scores = lax.dot_general(
                query, key_value, (((1,), (1,)), ((), ())), preferred_element_type=jnp.float32
            )
            scores = jnp.minimum(scores + bias, score_cap)
            lost = jnp.log(1.0 + jnp.exp(scores))
            own = scores - lost
            if masked:
                row_ids = lax.broadcasted_iota(jnp.int32, scores.shape, 0) + (row_start + link * chain)
                col_ids = lax.broadcasted_iota(jnp.int32, scores.shape, 1) + index * chunk
                allowed = col_ids < row_ids
                lost = jnp.where(allowed, lost, 0.0)
            behind = jnp.dot(lost.astype(jnp.bfloat16), after, preferred_element_type=jnp.float32)
            before = carry[place, :]
            weights = jnp.exp(own - (behind + before))
            if masked:
                weights = jnp.where(allowed, weights, 0.0)
            acc[place, :] += jnp.dot(
                weights.astype(jnp.bfloat16), key_value, preferred_element_type=jnp.float32
            )
            carry[place, :] = before + (behind[:, :1] + lost[:, :1])

    full = row_start // chunk
    top = (row_start + rows + chunk - 1) // chunk

    @pl.loop(0, top - full)
    def _(i):
        step(True, top - 1 - i)

    @pl.loop(0, full)
    def _(i):
        step(False, full - 1 - i)

    remain = jnp.broadcast_to(-carry[...], acc.shape)
    high = remain.astype(jnp.bfloat16)
    rest = remain - high.astype(jnp.float32)
    middle = rest.astype(jnp.bfloat16)
    low = (rest - middle.astype(jnp.float32)).astype(jnp.bfloat16)
    lane = lax.broadcasted_iota(jnp.int32, acc.shape, 1)
    packed = jnp.where(lane == 0, high.astype(jnp.float32), 0.0)
    packed = jnp.where(lane == 1, middle.astype(jnp.float32), packed)
    packed = jnp.where(lane == 2, low.astype(jnp.float32), packed)
    out_ref[0] = jnp.where(lane >= HEAD_DIM, acc[...], packed).astype(jnp.bfloat16)


def attend(received, bias_row, part, tok_dev):
    n_sp, _, lanes = received.shape
    share = received.shape[1] - tok_dev
    rows = min(512, share)
    chain = min(256, rows)
    tiles_block = share // rows
    bias3 = bias_row.reshape(n_sp * tok_dev // KEY_CHUNK, 1, KEY_CHUNK)
    pairs = n_sp * share * n_sp * tok_dev // 2
    return pl.pallas_call(
        functools.partial(attention_kernel, tok_dev, share, rows, chain),
        out_shape=jax.ShapeDtypeStruct((n_sp, share, lanes), jnp.bfloat16),
        grid_spec=pltpu.PrefetchScalarGridSpec(
            num_scalar_prefetch=1,
            grid=(n_sp * tiles_block,),
            in_specs=[
                pl.BlockSpec(received.shape, lambda i, part: (0, 0, 0)),
                pl.BlockSpec(bias3.shape, lambda i, part: (0, 0, 0)),
            ],
            out_specs=pl.BlockSpec((1, rows, lanes), lambda i, part: (i // tiles_block, i % tiles_block, 0)),
            scratch_shapes=[
                pltpu.VMEM((rows, lanes), jnp.float32),
                pltpu.VMEM((rows, 1), jnp.float32),
            ],
        ),
        compiler_params=pltpu.CompilerParams(
            dimension_semantics=("arbitrary",), vmem_limit_bytes=32 * 1024 * 1024
        ),
        cost_estimate=pl.CostEstimate(
            flops=pairs * (4 * lanes + 2 * KEY_CHUNK), bytes_accessed=received.size * 2, transcendentals=3 * pairs
        ),
    )(part, received, bias3)


def per_device(
    tokens,
    norm_gain,
    signal_proj,
    postgate_proj,
    pregate_proj,
    query_proj,
    key_proj,
    value_proj,
    filter_taps,
    break_bias,
    filter_readout,
    attention_readout,
):
    tok_dev = tokens.shape[0]
    heads_dev = break_bias.shape[1]
    n_sp = lax.axis_size("sp")
    parts = n_sp // heads_dev
    share = tok_dev // parts
    position = lax.axis_index("sp")
    all_bias = lax.all_gather(break_bias.T, "sp", axis=1, tiled=True)
    all_bias, tokens = lax.optimization_barrier((all_bias, tokens))
    bias_row = lax.dynamic_slice_in_dim(all_bias, position // parts, 1, 0).astype(jnp.float32)
    model = key_proj.shape[0]
    key_value_proj = jnp.concatenate(
        [
            key_proj.reshape(model, heads_dev, HEAD_DIM),
            value_proj.reshape(model, heads_dev, HEAD_DIM),
        ],
        axis=2,
    ).reshape(model, 2 * heads_dev * HEAD_DIM)
    whole_rows = lax.all_gather(tokens, "tp", axis=1, tiled=True)
    widened = whole_rows.astype(jnp.float32)
    inverse = lax.rsqrt(jnp.mean(widened * widened, axis=1) + epsilon)
    scaled = (widened * norm_gain[None, :]).astype(jnp.bfloat16)

    def project(weight, factor=1.0):
        product = jnp.dot(scaled, weight, preferred_element_type=jnp.float32)
        return (product * inverse[:, None]).astype(jnp.bfloat16) * jnp.bfloat16(factor)

    key_values = project(key_value_proj).reshape(tok_dev, heads_dev, 2 * HEAD_DIM)
    queries = project(query_proj, HEAD_DIM ** (-0.5)).reshape(tok_dev, heads_dev, HEAD_DIM)
    queries = jnp.pad(queries, ((0, 0), (0, 0), (0, HEAD_DIM)))
    key_values = key_values.transpose(1, 0, 2)
    queries = queries.transpose(1, 0, 2)
    outgoing = jnp.stack(
        [
            jnp.concatenate([key_values, queries[:, part * share : (part + 1) * share]], axis=1)
            for part in range(parts)
        ],
        axis=1,
    ).reshape(n_sp, tok_dev + share, 2 * HEAD_DIM)
    received = lax.all_to_all(outgoing, "sp", split_axis=0, concat_axis=0, tiled=True)
    signal, post_gate, pre_gate = (project(w) for w in (signal_proj, postgate_proj, pregate_proj))
    rim_width = CONV_W - 1
    rim_signal, rim_pre = passed_along(
        (signal[tok_dev - rim_width :], pre_gate[tok_dev - rim_width :]), "sp", 1
    )
    extended = jnp.concatenate(
        [
            rim_pre.astype(jnp.float32) * rim_signal.astype(jnp.float32),
            pre_gate.astype(jnp.float32) * signal.astype(jnp.float32),
        ],
        axis=0,
    )
    tap_values = filter_taps.astype(jnp.float32)
    running = jnp.zeros((tok_dev, extended.shape[1]), jnp.float32)
    for offset in range(CONV_W):
        running = running + tap_values[offset][None, :] * extended[offset : offset + tok_dev]
    filtered = (post_gate.astype(jnp.float32) * running).astype(jnp.bfloat16)
    filter_rows = lax.all_to_all(filtered, "tp", split_axis=0, concat_axis=1, tiled=True)

    part = (position % parts).astype(jnp.int32).reshape(1)
    computed = attend(received, bias_row, part, tok_dev)
    returned = lax.all_to_all(computed, "sp", split_axis=0, concat_axis=0, tiled=True)
    returned = returned.reshape(heads_dev, tok_dev, 2 * HEAD_DIM)
    attended = returned[:, :, HEAD_DIM:].transpose(1, 0, 2).reshape(tok_dev, heads_dev * HEAD_DIM)
    remain = jnp.sum(returned[:, :, :3].astype(jnp.float32), axis=2)
    mass_logarithm = jnp.log(jnp.maximum(-jnp.expm1(remain), mass_floor))
    attended_rows = lax.all_to_all(attended, "tp", split_axis=0, concat_axis=1, tiled=True)
    mixed = (
        jnp.dot(filter_rows, filter_readout, preferred_element_type=jnp.float32)
        + jnp.dot(attended_rows, attention_readout, preferred_element_type=jnp.float32)
    ).astype(jnp.bfloat16)
    return (mixed, mass_logarithm)


def tile_core(u):
    return jnp.where((u == 0) | (u == 3), 0, 1)


def tile_at(index, core):
    return (index // 2) * 4 + jnp.where(index % 2 == 0, core, 3 - core)


def scatter_matrix(rows_are_places, n):
    row = lax.broadcasted_iota(jnp.int32, (n, n), 0)
    col = lax.broadcasted_iota(jnp.int32, (n, n), 1)
    place, slot = (row, col) if rows_are_places else (col, row)
    span = n // 8
    hit = place == (slot % 8) * span + (span - 1 - slot // 8)
    return jnp.where(hit, 1.0, 0.0).astype(jnp.bfloat16)


def remote(src, dst, send, recv, sp, tp):
    return pltpu.make_async_remote_copy(
        src_ref=src,
        dst_ref=dst,
        send_sem=send,
        recv_sem=recv,
        device_id={"sp": sp, "tp": tp},
        device_id_type=pl.DeviceIdType.MESH,
    )


def meet(peers):
    barrier = pltpu.get_barrier_semaphore()
    for sp, tp in peers:
        pl.semaphore_signal(
            barrier, inc=1, device_id={"sp": sp, "tp": tp}, device_id_type=pl.DeviceIdType.MESH
        )
    pl.semaphore_wait(barrier, len(peers))


def mix_in_kernel(
    n_sp,
    heads,
    tokens,
    gain,
    signal_w,
    post_w,
    pre_w,
    query_w,
    key_w,
    value_w,
    taps,
    bias,
    gathered,
    filt,
    xbuf,
    scaled,
    inverse,
    weights,
    outgoing,
    product,
    rim,
    rim_out,
    ready,
    w_sem,
    own_sem,
    ag_send,
    ag_recv,
    kv_send,
    kv_recv,
    fwd_send,
    rim_sem,
    filt_send,
    filt_recv,
):
    p = lax.axis_index("sp")
    t = lax.axis_index("tp")
    y, c = t // 2, t % 2
    mate = 2 * y + 1 - c
    cross = 2 * (1 - y) + c
    cross_mate = 2 * (1 - y) + 1 - c
    tok_dev, shard = tokens.shape
    n_tp = xbuf.shape[0]
    size = tok_dev // n_tp
    width = key_w.shape[1]
    model = n_tp * shard
    primary = c == p // heads
    peers = [((p + k) % n_sp, t) for k in range(1, n_sp)] + [(p, (t + k) % n_tp) for k in range(1, n_tp)]

    sources = (key_w, query_w, value_w, signal_w, pre_w, post_w)
    loads = [pltpu.make_async_copy(w, weights.at[i], w_sem.at[i]) for i, w in enumerate(sources)]
    own = [
        pltpu.make_async_copy(
            tokens.at[pl.ds(i * size, size)], xbuf.at[t, pl.ds(i * size, size)], own_sem.at[i]
        )
        for i in range(n_tp)
    ]
    own[0].start()
    for load in loads[:3]:
        load.start()
    meet(peers)

    def token_copy(kind, i):
        rows = pl.ds(i * size, size)
        if kind == 0:
            return remote(tokens.at[rows], xbuf.at[t, rows], ag_send.at[0, i], ag_recv.at[0, i], p, cross)
        if kind == 1:
            return remote(tokens.at[rows], xbuf.at[t, rows], ag_send.at[1, i], ag_recv.at[1, i], p, mate)
        return remote(
            xbuf.at[cross, rows], xbuf.at[cross, rows], ag_send.at[2, i], ag_recv.at[2, i], p, mate
        )

    for i in range(n_tp):
        token_copy(0, i).start()
    for i in range(n_tp):
        token_copy(1, i).start()
    for copy in own[1:]:
        copy.start()
    for load in loads[3:]:
        load.start()
    for load in loads[:3]:
        load.wait()
    order = scatter_matrix(False, size)
    lane = lax.broadcasted_iota(jnp.int32, (size, 128), 1)
    step = 32

    def kv_copy(i, h):
        target = c * heads + h
        stays = target == p
        sp = jnp.where(stays, p, target)
        tp = jnp.where(stays, mate, t)
        return remote(
            outgoing.at[i, h], gathered.at[p, i], kv_send.at[i, h], kv_recv.at[p, i], sp, tp
        )

    @pl.loop(0, n_tp)
    def _(i):
        rows = pl.ds(pl.multiple_of(i * size, size), size)
        pltpu.make_async_copy(tokens.at[rows], xbuf.at[t, rows], own_sem.at[i]).wait()
        token_copy(0, i).wait_recv()
        token_copy(2, i).start()
        token_copy(1, i).wait_recv()
        token_copy(2, i).wait_recv()

        @pl.loop(0, size // step)
        def _(k):
            place = pl.ds(pl.multiple_of(i * size + k * step, step), step)
            total = jnp.zeros((step, 1), jnp.float32)
            for part in range(n_tp):
                x = xbuf[part, place, :].astype(jnp.float32)
                total = total + jnp.sum(x * x, axis=1, keepdims=True)
                columns = slice(part * shard, (part + 1) * shard)
                scaled[place, columns] = (x * gain[:, columns]).astype(jnp.bfloat16)
            inverse[place, :] = lax.rsqrt(total * (1.0 / model) + epsilon)

        x = scaled[rows, :]
        inv = inverse[rows, :]

        def project(index):
            y_ = jnp.dot(x, weights[index], preferred_element_type=jnp.float32)
            return (y_ * inv).astype(jnp.bfloat16)

        k_rows = jnp.dot(order, project(0), preferred_element_type=jnp.float32)
        q_rows = jnp.dot(order, project(1), preferred_element_type=jnp.float32) * (HEAD_DIM**-0.5)
        v_cols = jnp.dot(order, project(2), preferred_element_type=jnp.float32).T
        bias_rows = jnp.dot(order, bias[rows, :], preferred_element_type=jnp.float32)
        bias_rows = jnp.concatenate(
            [bias_rows, jnp.zeros((size, 128 - heads), jnp.float32)], axis=1
        ).T
        half = 2 * HEAD_DIM
        for h in range(heads):
            pair = slice((h // 2) * half, (h // 2 + 1) * half)
            kp, qp = k_rows[:, pair], q_rows[:, pair]
            if h % 2 == 0:
                kq = jnp.where(lane < HEAD_DIM, kp, pltpu.roll(qp, HEAD_DIM, 1))
            else:
                kq = jnp.where(lane < HEAD_DIM, pltpu.roll(kp, HEAD_DIM, 1), qp)
            kq = kq.astype(jnp.bfloat16)
            first = lax.broadcasted_iota(jnp.int32, (16, size), 0) == 0
            tail = jnp.where(first, bias_rows[h : h + 1, :], 0.0)
            vb = jnp.concatenate([v_cols[h * HEAD_DIM : (h + 1) * HEAD_DIM, :], tail], axis=0)
            vb = vb.astype(jnp.bfloat16)
            deep = HEAD_DIM + 16

            def put(ref):
                ref[0:size, :] = kq
                ref[size : size + deep, :] = vb[:, :128]
                ref[size + deep : size + 2 * deep, :] = vb[:, 128:]

            put(outgoing.at[i, h])

            @pl.when(c * heads + h == p)
            def _():
                put(gathered.at[p, i])

            kv_copy(i, h).start()

    for load in loads[3:]:
        load.wait()

    def gate(u):
        rows = pl.ds(u * size, size)
        x = scaled[rows, :]
        inv = inverse[rows, :]
        outs = []
        for index in range(3, 6):
            y_ = jnp.dot(x, weights[index], preferred_element_type=jnp.float32)
            outs.append((y_ * inv).astype(jnp.bfloat16))
        product[pl.ds(8 + u * size, size), :] = outs[1].astype(jnp.float32) * outs[0].astype(jnp.float32)
        ready[rows, :] = outs[2]

    gate(n_tp - 1)
    rim_out[...] = product[pl.ds(tok_dev, 8), :]
    rim_copy = remote(rim_out, rim, rim_sem.at[0], rim_sem.at[1], (p + 1) % n_sp, t)
    rim_copy.start()
    for u in range(n_tp - 1):
        gate(u)
    rim_copy.wait()
    product[0:8, :] = jnp.where(p > 0, rim[...], 0.0)
    tap_values = taps[...].astype(jnp.float32)

    def filt_copy(u):
        return remote(ready.at[pl.ds(u * size, size)], filt.at[t], filt_send.at[u], filt_recv.at[t], p, u)

    for u in range(n_tp):
        running = jnp.zeros((size, width), jnp.float32)
        for w in range(CONV_W):
            start = 8 - (CONV_W - 1) + w + u * size
            running = running + tap_values[w : w + 1, :] * product[pl.ds(start, size), :]
        rows = pl.ds(u * size, size)
        done = (ready[rows, :].astype(jnp.float32) * running).astype(jnp.bfloat16)
        ready[rows, :] = done

        @pl.when(t == u)
        def _():
            filt[u] = done

        @pl.when(t != u)
        def _():
            filt_copy(u).start()

    def arrival(b, i):
        return remote(outgoing.at[i, 0], gathered.at[b, i], fwd_send.at[b, i], kv_recv.at[b, i], p, mate)

    def forward(b, i):
        return remote(gathered.at[b, i], gathered.at[b, i], fwd_send.at[b, i], kv_recv.at[b, i], p, mate)

    @pl.when(primary)
    def _():
        @pl.loop(0, n_tp)
        def _(i):
            @pl.loop(1, n_sp)
            def _(k):
                b = (p + k) % n_sp
                arrival(b, i).wait_recv()
                forward(b, i).start()

        @pl.loop(0, n_tp)
        def _(i):
            @pl.loop(1, n_sp)
            def _(k):
                forward((p + k) % n_sp, i).wait_send()

    @pl.when(jnp.logical_not(primary))
    def _():
        @pl.loop(0, n_tp)
        def _(i):
            @pl.loop(0, n_sp)
            def _(b):
                arrival(b, i).wait_recv()

    for i in range(n_tp):
        for kind in range(3):
            token_copy(kind, i).wait_send()
        for h in range(heads):
            kv_copy(i, h).wait_send()
    for k in range(1, n_tp):
        u = (t + k) % n_tp
        remote(ready.at[pl.ds(0, size)], filt.at[u], filt_send.at[u], filt_recv.at[u], p, u).wait()


def mix_in(tokens, norm_gain, projections, taps, bias, n_sp, n_tp):
    tok_dev, shard = tokens.shape
    heads = bias.shape[1]
    width = projections[0].shape[1]
    model = n_tp * shard
    size = tok_dev // n_tp
    block = size + 2 * (HEAD_DIM + 16)
    vmem = pl.BlockSpec(memory_space=pltpu.VMEM)
    anywhere = pl.BlockSpec(memory_space=pl.ANY)
    dma = pltpu.SemaphoreType.DMA
    bf16, f32 = jnp.bfloat16, jnp.float32
    signal_w, post_w, pre_w, query_w, key_w, value_w = projections
    return pl.pallas_call(
        functools.partial(mix_in_kernel, n_sp, heads),
        out_shape=[
            jax.ShapeDtypeStruct((n_sp, n_tp, block, 128), bf16),
            jax.ShapeDtypeStruct((n_tp, size, width), bf16),
        ],
        in_specs=[anywhere, vmem] + [anywhere] * 6 + [vmem, vmem],
        out_specs=[vmem, vmem],
        scratch_shapes=[
            pltpu.VMEM((n_tp, tok_dev, shard), bf16),
            pltpu.VMEM((tok_dev, model), bf16),
            pltpu.VMEM((tok_dev, 1), f32),
            pltpu.VMEM((6, model, width), bf16),
            pltpu.VMEM((n_tp, heads, block, 128), bf16),
            pltpu.VMEM((tok_dev + 8, width), f32),
            pltpu.VMEM((8, width), f32),
            pltpu.VMEM((8, width), f32),
            pltpu.VMEM((tok_dev, width), bf16),
            dma((6,)),
            dma((n_tp,)),
            dma((3, n_tp)),
            dma((3, n_tp)),
            dma((n_tp, heads)),
            dma((n_sp, n_tp)),
            dma((n_sp, n_tp)),
            dma((2,)),
            dma((n_tp,)),
            dma((n_tp,)),
        ],
        compiler_params=pltpu.CompilerParams(
            collective_id=0, has_side_effects=True, vmem_limit_bytes=60 * 1024 * 1024
        ),
        name="mix_in",
    )(tokens, norm_gain.reshape(1, model), signal_w, post_w, pre_w, query_w, key_w, value_w, taps, bias)


def later_product(total):
    n = total.shape[0]
    row = lax.broadcasted_iota(jnp.int32, total.shape, 0)
    x = jnp.where(row < n - 1, pltpu.roll(total, n - 1, 0), 1.0)
    k = 1
    while k < n:
        x = x * jnp.where(row < n - k, pltpu.roll(x, n - k, 0), 1.0)
        k *= 2
    return x


def stick_kernel(got, out, mass, keys, quer, acc, carry, w0, w1, r0, r1):
    p = lax.axis_index("sp")
    core = lax.axis_index("tp") % 2
    n_sp, subs = got.shape[:2]
    size = quer.shape[1]
    deep = HEAD_DIM + 16
    n_tiles = quer.shape[0]
    groups = size // 8
    wb, rb = (w0, w1), (r0, r1)
    lane = lax.broadcasted_iota(jnp.int32, (size, 128), 1)
    unit = (lax.broadcasted_iota(jnp.int32, (16, 128), 0) == 0) & (
        lax.broadcasted_iota(jnp.int32, (16, 128), 1) == HEAD_DIM
    )
    unit = jnp.where(unit, 1.0, 0.0).astype(jnp.bfloat16)
    constant = jnp.where(lane == HEAD_DIM, 1.0, 0.0)

    @pl.loop(0, n_sp)
    def _(b):
        for i in range(subs):
            kq = got[b, i, 0:size, :]
            tail = jnp.concatenate(
                [
                    got[b, i, size + HEAD_DIM : size + deep, :],
                    got[b, i, size + deep + HEAD_DIM : size + 2 * deep, :],
                ],
                axis=1,
            )
            column = lax.dot_general(
                tail, unit, (((0,), (0,)), ((), ())), preferred_element_type=jnp.float32
            )
            keys[b, i] = jnp.where(lane < HEAD_DIM, kq.astype(jnp.float32), column).astype(jnp.bfloat16)

    @pl.loop(0, n_tiles)
    def _(index):
        tile = tile_at(index, core)
        rolled = pltpu.roll(got[tile // subs, tile % subs, 0:size, :].astype(jnp.float32), HEAD_DIM, 1)
        quer[index] = jnp.where(lane < HEAD_DIM, rolled, constant).astype(jnp.bfloat16)

    col = lax.broadcasted_iota(jnp.int32, (8, size), 1)
    place = (col % 8) * groups + (groups - 1) - col // 8
    segment = lax.broadcasted_iota(jnp.int32, (8, size), 0) * groups
    relative = place - segment

    def early(slot, index, b, masked):
        q = quer[index]
        tile = tile_at(index, core)
        for s in range(subs):
            scores = lax.dot_general(
                keys[b, s], q, (((1,), (1,)), ((), ())), preferred_element_type=jnp.float32
            )
            shift = (tile % subs - s) * size
            run = None
            for j in range(groups):
                e = jnp.exp(jnp.minimum(scores[8 * j : 8 * j + 8, :], score_cap_fast))
                if masked:
                    e = jnp.where(relative + shift > groups - 1 - j, e, 0.0)
                r = 1.0 / (1.0 + e)
                run = r if run is None else run * r
                w = e * run
                if j % 2:
                    pair = jnp.concatenate([before, w], axis=0).astype(jnp.bfloat16)
                    wb[slot][s, 8 * (j - 1) : 8 * (j + 1), :] = pair
                before = w
            rb[slot][s] = run

    def late(slot, index, b):
        first = b == tile_at(index, core) // subs
        running = jnp.where(first, 1.0, carry[...])
        total = jnp.where(first, 0.0, acc[...])
        for s in range(subs - 1, -1, -1):
            run = rb[slot][s]
            factor = later_product(run) * running
            running = jnp.broadcast_to((factor * run)[:1], run.shape)
            twice = jnp.concatenate([factor, factor], axis=0).astype(jnp.bfloat16)
            pieces = [wb[slot][s, 16 * j : 16 * j + 16, :] * twice for j in range(groups // 2)]
            values = jnp.concatenate(
                [got[b, s, size : size + HEAD_DIM, :], got[b, s, size + deep : size + deep + HEAD_DIM, :]],
                axis=1,
            )
            total = total + jnp.dot(
                values, jnp.concatenate(pieces, axis=0), preferred_element_type=jnp.float32
            )
        acc[...] = total
        carry[...] = running
        out[index] = total.astype(jnp.bfloat16)
        mass[index] = jnp.log(jnp.maximum(1.0 - running, mass_floor))

    def block_of(index):
        return tile_at(index, core) // subs

    items = 0
    for index in range(n_tiles):
        items = items + (index // 2) + 1
    steps = items + 1
    skip = steps % 2

    def half(z, m, state):
        i1, b1, i2, b2 = state

        def go(masked):
            late(z, i2, b2)
            early(1 - z, i1, b1, masked)

        lax.cond(b1 == block_of(i1), lambda: go(True), lambda: go(False))
        last = b1 == 0
        after = jnp.minimum(i1 + 1, n_tiles - 1)
        ni = jnp.where(last, after, i1)
        nb = jnp.where(last, block_of(after), b1 - 1)
        advance = m >= 0
        return jnp.where(advance, ni, i1), jnp.where(advance, nb, b1), i1, b1

    def body(k, state):
        for z in range(2):
            state = half(z, 2 * k + z - skip, state)
        return state

    zero = jnp.int32(0)
    lax.fori_loop(0, (steps + skip) // 2, body, (zero, zero, zero, zero))


def stick(gathered):
    n_sp, subs, block, _ = gathered.shape
    size = block - 2 * (HEAD_DIM + 16)
    n_tiles = n_sp * subs // 2
    vmem = pl.BlockSpec(memory_space=pltpu.VMEM)
    bf16, f32 = jnp.bfloat16, jnp.float32
    pairs = n_tiles * size * (n_sp + 1) * subs * size // 2
    return pl.pallas_call(
        stick_kernel,
        out_shape=[
            jax.ShapeDtypeStruct((n_tiles, HEAD_DIM, size), bf16),
            jax.ShapeDtypeStruct((n_tiles, 8, size), f32),
        ],
        in_specs=[vmem],
        out_specs=[vmem, vmem],
        scratch_shapes=[
            pltpu.VMEM((n_sp, subs, size, 128), bf16),
            pltpu.VMEM((n_tiles, size, 128), bf16),
            pltpu.VMEM((HEAD_DIM, size), f32),
            pltpu.VMEM((8, size), f32),
            pltpu.VMEM((subs, size, size), bf16),
            pltpu.VMEM((subs, size, size), bf16),
            pltpu.VMEM((subs, 8, size), f32),
            pltpu.VMEM((subs, 8, size), f32),
        ],
        compiler_params=pltpu.CompilerParams(vmem_limit_bytes=48 * 1024 * 1024),
        cost_estimate=pl.CostEstimate(
            flops=pairs * 4 * HEAD_DIM, bytes_accessed=gathered.size * 2, transcendentals=2 * pairs
        ),
        name="stick",
    )(gathered)


def mix_out_kernel(
    n_sp,
    heads,
    tiles,
    mass,
    filt,
    filter_w,
    attend_w,
    mixed,
    logs,
    arrived,
    marks,
    wf,
    wa,
    partial,
    attended,
    w_sem,
    a_send,
    a_recv,
    m_send,
    m_recv,
):
    p = lax.axis_index("sp")
    t = lax.axis_index("tp")
    y, c = t // 2, t % 2
    n_tp, size, width = filt.shape
    n_tiles = tiles.shape[0]
    owner = 2 * y + p // heads
    head = owner * heads + p % heads
    total_heads = arrived.shape[0]
    loads = [
        pltpu.make_async_copy(filter_w, wf, w_sem.at[0]),
        pltpu.make_async_copy(attend_w, wa, w_sem.at[1]),
    ]
    for load in loads:
        load.start()
    peers = []
    for a in range(n_sp):
        for b in range(n_tp):
            if a or b:
                peers.append(((p + a) % n_sp, (t + b) % n_tp))
    meet(peers)

    def tile_copy(index):
        tile = tile_at(index, c)
        b, u = tile // n_tp, tile % n_tp
        return remote(tiles.at[index], arrived.at[head], a_send.at[index], a_recv.at[head], b, u)

    def mark_copy(index):
        tile = tile_at(index, c)
        b, u = tile // n_tp, tile % n_tp
        slot = p % heads * n_tp + u
        return remote(mass.at[index], marks.at[slot], m_send.at[index], m_recv.at[slot], b, owner)

    def each(index, act):
        tile = tile_at(index, c)
        b, u = tile // n_tp, tile % n_tp
        own_tile = (b == p) & (u == t)
        own_mark = (b == p) & (owner == t)
        if act == "start":

            @pl.when(own_tile)
            def _():
                arrived[head] = tiles[index]

            @pl.when(own_mark)
            def _():
                marks[p % heads * n_tp + u] = mass[index]

        @pl.when(jnp.logical_not(own_tile))
        def _():
            copy = tile_copy(index)
            copy.start() if act == "start" else copy.wait_send()

        @pl.when(jnp.logical_not(own_mark))
        def _():
            copy = mark_copy(index)
            copy.start() if act == "start" else copy.wait_send()

    pl.loop(0, n_tiles)(lambda index: each(index, "start"))
    loads[0].wait()
    columns = 256

    @pl.loop(0, mixed.shape[1] // columns)
    def _(k):
        at = pl.ds(pl.multiple_of(k * columns, columns), columns)
        total = jnp.zeros((size, columns), jnp.float32)
        for part in range(n_tp):
            total = total + jnp.dot(
                filt[part], wf[part * width : (part + 1) * width, at], preferred_element_type=jnp.float32
            )
        partial[:, at] = total

    loads[1].wait()
    mine = tile_core(t) == c

    @pl.loop(0, total_heads)
    def _(k):
        @pl.when(jnp.logical_not((k == head) & mine))
        def _():
            remote(tiles.at[0], arrived.at[k], a_send.at[0], a_recv.at[k], p, t).wait_recv()

    order = scatter_matrix(True, size)
    for part in range(n_tp):
        stack = jnp.concatenate([arrived[part * heads + h] for h in range(heads)], axis=0)
        rows = lax.dot_general(order, stack, (((1,), (1,)), ((), ())), preferred_element_type=jnp.float32)
        attended[:, part * width : (part + 1) * width] = rows.astype(jnp.bfloat16)

    @pl.loop(0, mixed.shape[1] // columns)
    def _(k):
        at = pl.ds(pl.multiple_of(k * columns, columns), columns)
        total = partial[:, at] + jnp.dot(attended[...], wa[:, at], preferred_element_type=jnp.float32)
        mixed[:, at] = total.astype(jnp.bfloat16)

    @pl.loop(0, heads)
    def _(h):
        for u in range(n_tp):
            own = (p == c * heads + h) & (tile_core(u) == c)

            @pl.when(jnp.logical_not(own))
            def _():
                slot = h * n_tp + u
                remote(mass.at[0], marks.at[slot], m_send.at[0], m_recv.at[slot], p, t).wait_recv()

    back = scatter_matrix(False, size)
    for u in range(n_tp):
        row = lax.broadcasted_iota(jnp.int32, (8, size), 0)
        value = jnp.zeros((8, size), jnp.float32)
        for h in range(heads):
            value = jnp.where(row == h, marks[h * n_tp + u], value)
        total = jnp.zeros((8, size), jnp.float32)
        for _ in range(3):
            high = value.astype(jnp.bfloat16)
            value = value - high.astype(jnp.float32)
            total = total + jnp.dot(high, back, preferred_element_type=jnp.float32)
        logs[:, u * size : (u + 1) * size] = total[:heads]
    pl.loop(0, n_tiles)(lambda index: each(index, "wait"))


def mix_out(tiles, mass, filt, filter_readout, attention_readout, n_sp, heads):
    n_tp, size, width = filt.shape
    model = filter_readout.shape[1]
    vmem = pl.BlockSpec(memory_space=pltpu.VMEM)
    anywhere = pl.BlockSpec(memory_space=pl.ANY)
    dma = pltpu.SemaphoreType.DMA
    bf16, f32 = jnp.bfloat16, jnp.float32
    n_tiles = tiles.shape[0]
    return pl.pallas_call(
        functools.partial(mix_out_kernel, n_sp, heads),
        out_shape=[
            jax.ShapeDtypeStruct((size, model), bf16),
            jax.ShapeDtypeStruct((heads, n_tp * size), f32),
        ],
        in_specs=[vmem, vmem, vmem, anywhere, anywhere],
        out_specs=[vmem, vmem],
        scratch_shapes=[
            pltpu.VMEM((heads * n_tp, HEAD_DIM, size), bf16),
            pltpu.VMEM((heads * n_tp, 8, size), f32),
            pltpu.VMEM(filter_readout.shape, bf16),
            pltpu.VMEM(attention_readout.shape, bf16),
            pltpu.VMEM((size, model), f32),
            pltpu.VMEM((size, n_tp * width), bf16),
            dma((2,)),
            dma((n_tiles,)),
            dma((heads * n_tp,)),
            dma((n_tiles,)),
            dma((heads * n_tp,)),
        ],
        compiler_params=pltpu.CompilerParams(
            collective_id=1, has_side_effects=True, vmem_limit_bytes=60 * 1024 * 1024
        ),
        name="mix_out",
    )(tiles, mass, filt, filter_readout, attention_readout)


def per_device_fast(
    tokens,
    norm_gain,
    signal_proj,
    postgate_proj,
    pregate_proj,
    query_proj,
    key_proj,
    value_proj,
    filter_taps,
    break_bias,
    filter_readout,
    attention_readout,
):
    n_sp, n_tp = lax.axis_size("sp"), lax.axis_size("tp")
    projections = (signal_proj, postgate_proj, pregate_proj, query_proj, key_proj, value_proj)
    gathered, filt = mix_in(tokens, norm_gain, projections, filter_taps, break_bias, n_sp, n_tp)
    tiles, mass = stick(gathered)
    return mix_out(tiles, mass, filt, filter_readout, attention_readout, n_sp, break_bias.shape[1])


def per_device_any(*operands):
    tok_dev = operands[0].shape[0]
    heads_dev = operands[9].shape[1]
    n_sp, n_tp = lax.axis_size("sp"), lax.axis_size("tp")
    fast = n_tp == 4 and n_sp == 2 * heads_dev and tok_dev == n_tp * 256 and operands[6].shape[1] == 256
    return (per_device_fast if fast else per_device)(*operands)


def solution(mesh):
    placed = (
        P("sp", "tp"),
        P(),
        P(None, "tp"),
        P(None, "tp"),
        P(None, "tp"),
        P(None, "tp"),
        P(None, "tp"),
        P(None, "tp"),
        P(None, "tp"),
        P("sp", "tp"),
        P(),
        P(),
    )
    return jax.shard_map(
        per_device_any,
        mesh=mesh,
        in_specs=placed,
        out_specs=(P(("sp", "tp"), None), P("tp", "sp")),
        check_vma=False,
    )
```

```python
import functools

import jax
import jax.numpy as jnp
from jax import lax
from jax.experimental import pallas as pl
from jax.experimental.pallas import tpu as pltpu
from jax.sharding import PartitionSpec as P

HEAD_DIM = 64
CONV_W = 3
KEY_CHUNK = 256


epsilon = 1e-06
mass_floor = 0.1
score_cap = 88.0
score_cap_fast = 43.0


def passed_along(block, axis, distance):
    devices = range(lax.axis_size(axis))
    route = [(i - distance, i) for i in devices if i - distance in devices]
    return lax.ppermute(block, axis, route)


def attention_kernel(tok_dev, share, rows, chain, part_ref, recv_ref, bias_ref, out_ref, acc, carry):
    chunk = KEY_CHUNK
    tile = pl.program_id(0)
    tiles_block = share // rows
    block = tile // tiles_block
    inner = (tile % tiles_block) * rows
    row_start = block * tok_dev + part_ref[0] * share + inner
    chunks_block = tok_dev // chunk
    acc[...] = jnp.zeros_like(acc)
    carry[...] = jnp.zeros_like(carry)
    later = lax.broadcasted_iota(jnp.int32, (chunk, chunk), 0)
    earlier = lax.broadcasted_iota(jnp.int32, (chunk, chunk), 1)
    after = jnp.where(later > earlier, 1.0, 0.0).astype(jnp.bfloat16)

    def step(masked, index):
        offset = pl.multiple_of((index % chunks_block) * chunk, chunk)
        key_value = recv_ref[index // chunks_block, pl.ds(offset, chunk), :]
        bias = bias_ref[index]
        for link in range(rows // chain):
            place = pl.ds(link * chain, chain)
            query_place = pl.multiple_of(tok_dev + inner + link * chain, chain)
            query = recv_ref[block, pl.ds(query_place, chain), :]
            scores = lax.dot_general(
                query, key_value, (((1,), (1,)), ((), ())), preferred_element_type=jnp.float32
            )
            scores = jnp.minimum(scores + bias, score_cap)
            lost = jnp.log(1.0 + jnp.exp(scores))
            own = scores - lost
            if masked:
                row_ids = lax.broadcasted_iota(jnp.int32, scores.shape, 0) + (row_start + link * chain)
                col_ids = lax.broadcasted_iota(jnp.int32, scores.shape, 1) + index * chunk
                allowed = col_ids < row_ids
                lost = jnp.where(allowed, lost, 0.0)
            behind = jnp.dot(lost.astype(jnp.bfloat16), after, preferred_element_type=jnp.float32)
            before = carry[place, :]
            weights = jnp.exp(own - (behind + before))
            if masked:
                weights = jnp.where(allowed, weights, 0.0)
            acc[place, :] += jnp.dot(
                weights.astype(jnp.bfloat16), key_value, preferred_element_type=jnp.float32
            )
            carry[place, :] = before + (behind[:, :1] + lost[:, :1])

    full = row_start // chunk
    top = (row_start + rows + chunk - 1) // chunk

    @pl.loop(0, top - full)
    def _(i):
        step(True, top - 1 - i)

    @pl.loop(0, full)
    def _(i):
        step(False, full - 1 - i)

    remain = jnp.broadcast_to(-carry[...], acc.shape)
    high = remain.astype(jnp.bfloat16)
    rest = remain - high.astype(jnp.float32)
    middle = rest.astype(jnp.bfloat16)
    low = (rest - middle.astype(jnp.float32)).astype(jnp.bfloat16)
    lane = lax.broadcasted_iota(jnp.int32, acc.shape, 1)
    packed = jnp.where(lane == 0, high.astype(jnp.float32), 0.0)
    packed = jnp.where(lane == 1, middle.astype(jnp.float32), packed)
    packed = jnp.where(lane == 2, low.astype(jnp.float32), packed)
    out_ref[0] = jnp.where(lane >= HEAD_DIM, acc[...], packed).astype(jnp.bfloat16)


def attend(received, bias_row, part, tok_dev):
    n_sp, _, lanes = received.shape
    share = received.shape[1] - tok_dev
    rows = min(512, share)
    chain = min(256, rows)
    tiles_block = share // rows
    bias3 = bias_row.reshape(n_sp * tok_dev // KEY_CHUNK, 1, KEY_CHUNK)
    pairs = n_sp * share * n_sp * tok_dev // 2
    return pl.pallas_call(
        functools.partial(attention_kernel, tok_dev, share, rows, chain),
        out_shape=jax.ShapeDtypeStruct((n_sp, share, lanes), jnp.bfloat16),
        grid_spec=pltpu.PrefetchScalarGridSpec(
            num_scalar_prefetch=1,
            grid=(n_sp * tiles_block,),
            in_specs=[
                pl.BlockSpec(received.shape, lambda i, part: (0, 0, 0)),
                pl.BlockSpec(bias3.shape, lambda i, part: (0, 0, 0)),
            ],
            out_specs=pl.BlockSpec((1, rows, lanes), lambda i, part: (i // tiles_block, i % tiles_block, 0)),
            scratch_shapes=[
                pltpu.VMEM((rows, lanes), jnp.float32),
                pltpu.VMEM((rows, 1), jnp.float32),
            ],
        ),
        compiler_params=pltpu.CompilerParams(
            dimension_semantics=("arbitrary",), vmem_limit_bytes=32 * 1024 * 1024
        ),
        cost_estimate=pl.CostEstimate(
            flops=pairs * (4 * lanes + 2 * KEY_CHUNK), bytes_accessed=received.size * 2, transcendentals=3 * pairs
        ),
    )(part, received, bias3)


def per_device(
    tokens,
    norm_gain,
    signal_proj,
    postgate_proj,
    pregate_proj,
    query_proj,
    key_proj,
    value_proj,
    filter_taps,
    break_bias,
    filter_readout,
    attention_readout,
):
    tok_dev = tokens.shape[0]
    heads_dev = break_bias.shape[1]
    n_sp = lax.axis_size("sp")
    parts = n_sp // heads_dev
    share = tok_dev // parts
    position = lax.axis_index("sp")
    all_bias = lax.all_gather(break_bias.T, "sp", axis=1, tiled=True)
    all_bias, tokens = lax.optimization_barrier((all_bias, tokens))
    bias_row = lax.dynamic_slice_in_dim(all_bias, position // parts, 1, 0).astype(jnp.float32)
    model = key_proj.shape[0]
    key_value_proj = jnp.concatenate(
        [
            key_proj.reshape(model, heads_dev, HEAD_DIM),
            value_proj.reshape(model, heads_dev, HEAD_DIM),
        ],
        axis=2,
    ).reshape(model, 2 * heads_dev * HEAD_DIM)
    whole_rows = lax.all_gather(tokens, "tp", axis=1, tiled=True)
    widened = whole_rows.astype(jnp.float32)
    inverse = lax.rsqrt(jnp.mean(widened * widened, axis=1) + epsilon)
    scaled = (widened * norm_gain[None, :]).astype(jnp.bfloat16)

    def project(weight, factor=1.0):
        product = jnp.dot(scaled, weight, preferred_element_type=jnp.float32)
        return (product * inverse[:, None]).astype(jnp.bfloat16) * jnp.bfloat16(factor)

    key_values = project(key_value_proj).reshape(tok_dev, heads_dev, 2 * HEAD_DIM)
    queries = project(query_proj, HEAD_DIM ** (-0.5)).reshape(tok_dev, heads_dev, HEAD_DIM)
    queries = jnp.pad(queries, ((0, 0), (0, 0), (0, HEAD_DIM)))
    key_values = key_values.transpose(1, 0, 2)
    queries = queries.transpose(1, 0, 2)
    outgoing = jnp.stack(
        [
            jnp.concatenate([key_values, queries[:, part * share : (part + 1) * share]], axis=1)
            for part in range(parts)
        ],
        axis=1,
    ).reshape(n_sp, tok_dev + share, 2 * HEAD_DIM)
    received = lax.all_to_all(outgoing, "sp", split_axis=0, concat_axis=0, tiled=True)
    signal, post_gate, pre_gate = (project(w) for w in (signal_proj, postgate_proj, pregate_proj))
    rim_width = CONV_W - 1
    rim_signal, rim_pre = passed_along(
        (signal[tok_dev - rim_width :], pre_gate[tok_dev - rim_width :]), "sp", 1
    )
    extended = jnp.concatenate(
        [
            rim_pre.astype(jnp.float32) * rim_signal.astype(jnp.float32),
            pre_gate.astype(jnp.float32) * signal.astype(jnp.float32),
        ],
        axis=0,
    )
    tap_values = filter_taps.astype(jnp.float32)
    running = jnp.zeros((tok_dev, extended.shape[1]), jnp.float32)
    for offset in range(CONV_W):
        running = running + tap_values[offset][None, :] * extended[offset : offset + tok_dev]
    filtered = (post_gate.astype(jnp.float32) * running).astype(jnp.bfloat16)
    filter_rows = lax.all_to_all(filtered, "tp", split_axis=0, concat_axis=1, tiled=True)

    part = (position % parts).astype(jnp.int32).reshape(1)
    computed = attend(received, bias_row, part, tok_dev)
    returned = lax.all_to_all(computed, "sp", split_axis=0, concat_axis=0, tiled=True)
    returned = returned.reshape(heads_dev, tok_dev, 2 * HEAD_DIM)
    attended = returned[:, :, HEAD_DIM:].transpose(1, 0, 2).reshape(tok_dev, heads_dev * HEAD_DIM)
    remain = jnp.sum(returned[:, :, :3].astype(jnp.float32), axis=2)
    mass_logarithm = jnp.log(jnp.maximum(-jnp.expm1(remain), mass_floor))
    attended_rows = lax.all_to_all(attended, "tp", split_axis=0, concat_axis=1, tiled=True)
    mixed = (
        jnp.dot(filter_rows, filter_readout, preferred_element_type=jnp.float32)
        + jnp.dot(attended_rows, attention_readout, preferred_element_type=jnp.float32)
    ).astype(jnp.bfloat16)
    return (mixed, mass_logarithm)


def tile_core(u):
    return jnp.where((u == 0) | (u == 3), 0, 1)


def tile_at(index, core):
    return (index // 2) * 4 + jnp.where(index % 2 == 0, core, 3 - core)


def scatter_matrix(rows_are_places, n):
    row = lax.broadcasted_iota(jnp.int32, (n, n), 0)
    col = lax.broadcasted_iota(jnp.int32, (n, n), 1)
    place, slot = (row, col) if rows_are_places else (col, row)
    span = n // 8
    hit = place == (slot % 8) * span + (span - 1 - slot // 8)
    return jnp.where(hit, 1.0, 0.0).astype(jnp.bfloat16)


def remote(src, dst, send, recv, sp, tp):
    return pltpu.make_async_remote_copy(
        src_ref=src,
        dst_ref=dst,
        send_sem=send,
        recv_sem=recv,
        device_id={"sp": sp, "tp": tp},
        device_id_type=pl.DeviceIdType.MESH,
    )


def meet(peers):
    barrier = pltpu.get_barrier_semaphore()
    for sp, tp in peers:
        pl.semaphore_signal(
            barrier, inc=1, device_id={"sp": sp, "tp": tp}, device_id_type=pl.DeviceIdType.MESH
        )
    pl.semaphore_wait(barrier, len(peers))


def later_product(total):
    n = total.shape[0]
    row = lax.broadcasted_iota(jnp.int32, total.shape, 0)
    x = jnp.where(row < n - 1, pltpu.roll(total, n - 1, 0), 1.0)
    k = 1
    while k < n:
        x = x * jnp.where(row < n - k, pltpu.roll(x, n - k, 0), 1.0)
        k *= 2
    return x


def layer_kernel(
    n_sp,
    heads,
    tokens,
    gain,
    signal_w,
    post_w,
    pre_w,
    query_w,
    key_w,
    value_w,
    taps,
    bias,
    filter_w,
    attend_w,
    mixed,
    logs,
    xbuf,
    scaled,
    inverse,
    weights,
    outgoing,
    gathered,
    product,
    rim,
    rim_out,
    ready,
    filt,
    keys,
    quer,
    acc,
    carry,
    w0,
    w1,
    r0,
    r1,
    tiles,
    mass,
    arrived,
    marks,
    wf,
    wa,
    partial,
    attended,
    w_sem,
    own_sem,
    ag_send,
    ag_recv,
    kv_send,
    kv_recv,
    fwd_send,
    rim_sem,
    filt_send,
    filt_recv,
    a_send,
    a_recv,
    m_send,
    m_recv,
):
    p = lax.axis_index("sp")
    t = lax.axis_index("tp")
    y, c = t // 2, t % 2
    mate = 2 * y + 1 - c
    cross = 2 * (1 - y) + c
    tok_dev, shard = tokens.shape
    n_tp = xbuf.shape[0]
    size = tok_dev // n_tp
    width = key_w.shape[1]
    model = n_tp * shard
    half_sp = n_sp // 2
    upper = p // half_sp
    primary = c == p // heads
    owner = 2 * y + p // heads
    head = owner * heads + p % heads
    total_heads = arrived.shape[0]
    n_tiles = tiles.shape[0]
    groups = size // 8

    sources = (key_w, query_w, value_w, signal_w, pre_w, post_w)
    loads = [pltpu.make_async_copy(w, weights.at[i], w_sem.at[i]) for i, w in enumerate(sources)]
    loads.append(pltpu.make_async_copy(filter_w, wf, w_sem.at[6]))
    loads.append(pltpu.make_async_copy(attend_w, wa, w_sem.at[7]))
    own = [
        pltpu.make_async_copy(
            tokens.at[pl.ds(i * size, size)], xbuf.at[t, pl.ds(i * size, size)], own_sem.at[i]
        )
        for i in range(n_tp)
    ]
    own[0].start()
    for load in loads[:3]:
        load.start()
    peers = []
    for a in range(n_sp):
        for b in range(n_tp):
            if a or b:
                peers.append(((p + a) % n_sp, (t + b) % n_tp))
    meet(peers)

    def token_copy(kind, i):
        rows = pl.ds(i * size, size)
        if kind == 0:
            return remote(tokens.at[rows], xbuf.at[t, rows], ag_send.at[0, i], ag_recv.at[0, i], p, cross)
        if kind == 1:
            return remote(tokens.at[rows], xbuf.at[t, rows], ag_send.at[1, i], ag_recv.at[1, i], p, mate)
        return remote(
            xbuf.at[cross, rows], xbuf.at[cross, rows], ag_send.at[2, i], ag_recv.at[2, i], p, mate
        )

    for i in range(n_tp):
        token_copy(0, i).start()
    for i in range(n_tp):
        token_copy(1, i).start()
    for copy in own[1:]:
        copy.start()
    for load in loads[3:]:
        load.start()
    for load in loads[:3]:
        load.wait()
    order = scatter_matrix(False, size)
    back = scatter_matrix(True, size)
    lane = lax.broadcasted_iota(jnp.int32, (size, 128), 1)
    step = 32

    def kv_copy(i, h):
        target = c * heads + h
        stays = target == p
        sp = jnp.where(stays, p, target)
        tp = jnp.where(stays, mate, t)
        return remote(
            outgoing.at[i, h], gathered.at[p, i], kv_send.at[i, h], kv_recv.at[p, i], sp, tp
        )

    @pl.loop(0, n_tp)
    def _(i):
        rows = pl.ds(pl.multiple_of(i * size, size), size)
        pltpu.make_async_copy(tokens.at[rows], xbuf.at[t, rows], own_sem.at[i]).wait()
        token_copy(0, i).wait_recv()
        token_copy(2, i).start()
        token_copy(1, i).wait_recv()
        token_copy(2, i).wait_recv()

        @pl.loop(0, size // step)
        def _(k):
            place = pl.ds(pl.multiple_of(i * size + k * step, step), step)
            total = jnp.zeros((step, 1), jnp.float32)
            for part in range(n_tp):
                x = xbuf[part, place, :].astype(jnp.float32)
                total = total + jnp.sum(x * x, axis=1, keepdims=True)
                columns = slice(part * shard, (part + 1) * shard)
                scaled[place, columns] = (x * gain[:, columns]).astype(jnp.bfloat16)
            inverse[place, :] = lax.rsqrt(total * (1.0 / model) + epsilon)

        x = scaled[rows, :]
        inv = inverse[rows, :]

        def project(index):
            y_ = jnp.dot(x, weights[index], preferred_element_type=jnp.float32)
            return (y_ * inv).astype(jnp.bfloat16)

        k_rows = jnp.dot(order, project(0), preferred_element_type=jnp.float32)
        q_rows = jnp.dot(order, project(1), preferred_element_type=jnp.float32) * (HEAD_DIM**-0.5)
        v_cols = jnp.dot(order, project(2), preferred_element_type=jnp.float32).T
        bias_rows = jnp.dot(bias[:, rows], back, preferred_element_type=jnp.float32)
        pair_width = 2 * HEAD_DIM
        for h in range(heads):
            pair = slice((h // 2) * pair_width, (h // 2 + 1) * pair_width)
            kp, qp = k_rows[:, pair], q_rows[:, pair]
            if h % 2 == 0:
                kq = jnp.where(lane < HEAD_DIM, kp, pltpu.roll(qp, HEAD_DIM, 1))
            else:
                kq = jnp.where(lane < HEAD_DIM, pltpu.roll(kp, HEAD_DIM, 1), qp)
            kq = kq.astype(jnp.bfloat16)
            vb = v_cols[h * HEAD_DIM : (h + 1) * HEAD_DIM, :].astype(jnp.bfloat16)
            row = lax.broadcasted_iota(jnp.int32, (16, 128), 0)
            tail = jnp.where(row == 0, bias_rows[h : h + 1, :128], 0.0)
            tail = jnp.where(row == 1, bias_rows[h : h + 1, 128:], tail).astype(jnp.bfloat16)

            def put(ref):
                ref[0:size, :] = kq
                ref[size : size + HEAD_DIM, :] = vb[:, :128]
                ref[size + HEAD_DIM : size + 2 * HEAD_DIM, :] = vb[:, 128:]
                ref[size + 2 * HEAD_DIM :, :] = tail

            put(outgoing.at[i, h])

            @pl.when(c * heads + h == p)
            def _():
                put(gathered.at[p, i])

            kv_copy(i, h).start()

    for load in loads[3:6]:
        load.wait()

    def gate(u):
        rows = pl.ds(u * size, size)
        x = scaled[rows, :]
        inv = inverse[rows, :]
        outs = []
        for index in range(3, 6):
            y_ = jnp.dot(x, weights[index], preferred_element_type=jnp.float32)
            outs.append((y_ * inv).astype(jnp.bfloat16))
        product[pl.ds(8 + u * size, size), :] = outs[1].astype(jnp.float32) * outs[0].astype(jnp.float32)
        ready[rows, :] = outs[2]

    gate(n_tp - 1)
    rim_out[...] = product[pl.ds(tok_dev, 8), :]
    rim_copy = remote(rim_out, rim, rim_sem.at[0], rim_sem.at[1], (p + 1) % n_sp, t)
    rim_copy.start()
    for u in range(n_tp - 1):
        gate(u)
    rim_copy.wait()
    product[0:8, :] = jnp.where(p > 0, rim[...], 0.0)
    tap_values = taps[...].astype(jnp.float32)

    def filt_copy(u):
        return remote(ready.at[pl.ds(u * size, size)], filt.at[t], filt_send.at[u], filt_recv.at[t], p, u)

    for u in range(n_tp):
        running = jnp.zeros((size, width), jnp.float32)
        for w in range(CONV_W):
            start = 8 - (CONV_W - 1) + w + u * size
            running = running + tap_values[w : w + 1, :] * product[pl.ds(start, size), :]
        rows = pl.ds(u * size, size)
        done = (ready[rows, :].astype(jnp.float32) * running).astype(jnp.bfloat16)
        ready[rows, :] = done

        @pl.when(t == u)
        def _():
            filt[u] = done

        @pl.when(t != u)
        def _():
            filt_copy(u).start()

    row16 = lax.broadcasted_iota(jnp.int32, (16, 128), 0)
    lane16 = lax.broadcasted_iota(jnp.int32, (16, 128), 1)
    units = [
        jnp.where((row16 == k) & (lane16 == HEAD_DIM), 1.0, 0.0).astype(jnp.bfloat16) for k in range(2)
    ]
    constant = jnp.where(lane == HEAD_DIM, 1.0, 0.0)

    def arrival(b, i):
        return remote(outgoing.at[i, 0], gathered.at[b, i], fwd_send.at[b, i], kv_recv.at[b, i], p, mate)

    def forward(b, i):
        return remote(gathered.at[b, i], gathered.at[b, i], fwd_send.at[b, i], kv_recv.at[b, i], p, mate)

    def take(base):
        @pl.loop(0, n_tp)
        def _(i):
            @pl.loop(0, half_sp)
            def _(k):
                b = base + k

                @pl.when(jnp.logical_not(primary & (b == p)))
                def _():
                    arrival(b, i).wait_recv()

                @pl.when(primary & (b != p))
                def _():
                    forward(b, i).start()

                kq = gathered[b, i, 0:size, :].astype(jnp.float32)
                tail = gathered[b, i, size + 2 * HEAD_DIM :, :]
                column = jnp.concatenate(
                    [
                        lax.dot_general(
                            tail, unit, (((0,), (0,)), ((), ())), preferred_element_type=jnp.float32
                        )
                        for unit in units
                    ],
                    axis=0,
                )
                keys[b, i] = jnp.where(lane < HEAD_DIM, kq, column).astype(jnp.bfloat16)

                @pl.when(tile_core(i) == c)
                def _():
                    index = b * (n_tp // 2) + i // 2
                    rolled = pltpu.roll(kq, HEAD_DIM, 1)
                    quer[index] = jnp.where(lane < HEAD_DIM, rolled, constant).astype(jnp.bfloat16)

    col = lax.broadcasted_iota(jnp.int32, (8, size), 1)
    place8 = (col % 8) * groups + (groups - 1) - col // 8
    relative = place8 - lax.broadcasted_iota(jnp.int32, (8, size), 0) * groups
    wb, rb = (w0, w1), (r0, r1)

    def early(slot, index, b, masked):
        q = quer[index]
        tile = tile_at(index, c)
        for s in range(n_tp):
            scores = lax.dot_general(
                keys[b, s], q, (((1,), (1,)), ((), ())), preferred_element_type=jnp.float32
            )
            shift = (tile % n_tp - s) * size
            run = None
            for j in range(groups):
                e = jnp.exp(jnp.minimum(scores[8 * j : 8 * j + 8, :], score_cap_fast))
                if masked:
                    e = jnp.where(relative + shift > groups - 1 - j, e, 0.0)
                r = 1.0 / (1.0 + e)
                run = r if run is None else run * r
                w = e * run
                if j % 2:
                    pair = jnp.concatenate([before, w], axis=0).astype(jnp.bfloat16)
                    wb[slot][s, 8 * (j - 1) : 8 * (j + 1), :] = pair
                before = w
            rb[slot][s] = run

    def late(slot, index, b):
        first = b == tile_at(index, c) // n_tp
        running = jnp.where(first, 1.0, carry[index])
        total = jnp.where(first, 0.0, acc[index])
        for s in range(n_tp - 1, -1, -1):
            run = rb[slot][s]
            factor = later_product(run) * running
            running = jnp.broadcast_to((factor * run)[:1], run.shape)
            twice = jnp.concatenate([factor, factor], axis=0).astype(jnp.bfloat16)
            pieces = [wb[slot][s, 16 * j : 16 * j + 16, :] * twice for j in range(groups // 2)]
            values = jnp.concatenate(
                [
                    gathered[b, s, size : size + HEAD_DIM, :],
                    gathered[b, s, size + HEAD_DIM : size + 2 * HEAD_DIM, :],
                ],
                axis=1,
            )
            total = total + jnp.dot(
                values, jnp.concatenate(pieces, axis=0), preferred_element_type=jnp.float32
            )
        acc[index] = total
        carry[index] = running

    def tile_copy(index):
        tile = tile_at(index, c)
        b, u = tile // n_tp, tile % n_tp
        return remote(tiles.at[index], arrived.at[head], a_send.at[index], a_recv.at[head], b, u)

    def mark_copy(index):
        tile = tile_at(index, c)
        b, u = tile // n_tp, tile % n_tp
        slot = p % heads * n_tp + u
        return remote(mass.at[index], marks.at[slot], m_send.at[index], m_recv.at[slot], b, owner)

    def ownership(index):
        tile = tile_at(index, c)
        b, u = tile // n_tp, tile % n_tp
        return u, (b == p) & (u == t), (b == p) & (owner == t)

    def hand_over(index):
        u, own_tile, own_mark = ownership(index)
        value = acc[index].astype(jnp.bfloat16)
        mark = jnp.log(jnp.maximum(1.0 - carry[index], mass_floor))
        tiles[index] = value
        mass[index] = mark

        @pl.when(own_tile)
        def _():
            arrived[head] = value

        @pl.when(jnp.logical_not(own_tile))
        def _():
            tile_copy(index).start()

        @pl.when(own_mark)
        def _():
            marks[p % heads * n_tp + u] = mark

        @pl.when(jnp.logical_not(own_mark))
        def _():
            mark_copy(index).start()

    half_tiles = n_tiles // 2
    per_block = n_tp // 2

    def block_of(index):
        return tile_at(index, c) // n_tp

    def sweep(base, from_diagonal, low, items, sends):
        steps = items + 1
        skip = steps % 2
        spare = jnp.int32(n_tiles)

        def start_of(index):
            return jnp.where(from_diagonal, block_of(index), half_sp - 1)

        def half(z, m, state):
            i1, b1, i2, b2 = state

            def go(masked):
                late(z, i2, b2)
                early(1 - z, i1, b1, masked)

            lax.cond(b1 == block_of(i1), lambda: go(True), lambda: go(False))

            @pl.when(sends & (b2 == 0) & (m >= 1))
            def _():
                hand_over(i2)

            last = b1 == low
            after = jnp.minimum(i1 + 1, base + half_tiles - 1)
            ni = jnp.where(last, after, i1)
            nb = jnp.where(last, start_of(after), b1 - 1)
            advance = m >= 0
            return (
                jnp.where(advance, ni, i1),
                jnp.where(advance, nb, b1),
                jnp.where(advance, i1, spare),
                b1,
            )

        def body(k, state):
            for z in range(2):
                state = half(z, 2 * k + z - skip, state)
            return state

        first = start_of(base)
        rounds = jnp.where(items > 0, (steps + skip) // 2, 0)
        lax.fori_loop(0, rounds, body, (base, first, spare, first))

    triangle = per_block * (half_sp * (half_sp + 1) // 2)
    square = per_block * half_sp * half_sp
    is_upper = upper == 1

    @pl.loop(0, 3)
    def _(phase):
        near = phase == 0

        @pl.when(near)
        def _():
            take(upper * half_sp)

        @pl.when(phase == 1)
        def _():
            loads[6].wait()
            for k in range(1, n_tp):
                u = (t + k) % n_tp
                remote(ready.at[pl.ds(0, size)], filt.at[u], filt_send.at[u], filt_recv.at[u], p, u).wait()

            @pl.loop(0, model // 256)
            def _(k):
                at = pl.ds(pl.multiple_of(k * 256, 256), 256)
                total = jnp.zeros((size, 256), jnp.float32)
                for part in range(n_tp):
                    total = total + jnp.dot(
                        filt[part],
                        wf[part * width : (part + 1) * width, at],
                        preferred_element_type=jnp.float32,
                    )
                partial[:, at] = total

            take((1 - upper) * half_sp)

        first_items = jnp.where(is_upper, square, triangle + square)
        last_items = jnp.where(is_upper, triangle, 0)
        sweep(
            jnp.where(near, upper * half_tiles, jnp.where(phase == 1, half_tiles, 0)),
            jnp.logical_not(is_upper & (phase == 1)),
            jnp.where(near, upper * half_sp, 0),
            jnp.where(near, triangle, jnp.where(phase == 1, first_items, last_items)),
            jnp.logical_not(near & is_upper),
        )

    loads[7].wait()
    mine = tile_core(t) == c

    @pl.loop(0, total_heads)
    def _(k):
        @pl.when(jnp.logical_not((k == head) & mine))
        def _():
            remote(tiles.at[0], arrived.at[k], a_send.at[0], a_recv.at[k], p, t).wait_recv()

    for part in range(n_tp):
        stack = jnp.concatenate([arrived[part * heads + h] for h in range(heads)], axis=0)
        rows = lax.dot_general(back, stack, (((1,), (1,)), ((), ())), preferred_element_type=jnp.float32)
        attended[:, part * width : (part + 1) * width] = rows.astype(jnp.bfloat16)

    @pl.loop(0, model // 256)
    def _(k):
        at = pl.ds(pl.multiple_of(k * 256, 256), 256)
        total = partial[:, at] + jnp.dot(attended[...], wa[:, at], preferred_element_type=jnp.float32)
        mixed[:, at] = total.astype(jnp.bfloat16)

    @pl.loop(0, heads)
    def _(h):
        for u in range(n_tp):
            own_mark = (p == c * heads + h) & (tile_core(u) == c)

            @pl.when(jnp.logical_not(own_mark))
            def _():
                slot = h * n_tp + u
                remote(mass.at[0], marks.at[slot], m_send.at[0], m_recv.at[slot], p, t).wait_recv()

    for u in range(n_tp):
        row = lax.broadcasted_iota(jnp.int32, (8, size), 0)
        value = jnp.zeros((8, size), jnp.float32)
        for h in range(heads):
            value = jnp.where(row == h, marks[h * n_tp + u], value)
        total = jnp.zeros((8, size), jnp.float32)
        for _ in range(3):
            high = value.astype(jnp.bfloat16)
            value = value - high.astype(jnp.float32)
            total = total + jnp.dot(high, order, preferred_element_type=jnp.float32)
        logs[:, u * size : (u + 1) * size] = total[:heads]

    @pl.loop(0, n_tiles)
    def _(index):
        u, own_tile, own_mark = ownership(index)

        @pl.when(jnp.logical_not(own_tile))
        def _():
            tile_copy(index).wait_send()

        @pl.when(jnp.logical_not(own_mark))
        def _():
            mark_copy(index).wait_send()

    @pl.when(primary)
    def _():
        @pl.loop(0, n_tp)
        def _(i):
            @pl.loop(1, n_sp)
            def _(k):
                forward((p + k) % n_sp, i).wait_send()

    for i in range(n_tp):
        for kind in range(3):
            token_copy(kind, i).wait_send()
        for h in range(heads):
            kv_copy(i, h).wait_send()


def per_device_fast(
    tokens,
    norm_gain,
    signal_proj,
    postgate_proj,
    pregate_proj,
    query_proj,
    key_proj,
    value_proj,
    filter_taps,
    break_bias,
    filter_readout,
    attention_readout,
):
    n_sp, n_tp = lax.axis_size("sp"), lax.axis_size("tp")
    tok_dev, shard = tokens.shape
    heads = break_bias.shape[1]
    width = key_proj.shape[1]
    model = n_tp * shard
    size = tok_dev // n_tp
    block = size + 2 * HEAD_DIM + 16
    n_tiles = n_sp * n_tp // 2
    vmem = pl.BlockSpec(memory_space=pltpu.VMEM)
    anywhere = pl.BlockSpec(memory_space=pl.ANY)
    dma = pltpu.SemaphoreType.DMA
    bf16, f32 = jnp.bfloat16, jnp.float32
    return pl.pallas_call(
        functools.partial(layer_kernel, n_sp, heads),
        out_shape=[
            jax.ShapeDtypeStruct((size, model), bf16),
            jax.ShapeDtypeStruct((heads, tok_dev), f32),
        ],
        in_specs=[anywhere, vmem] + [anywhere] * 6 + [vmem, vmem, anywhere, anywhere],
        out_specs=[vmem, vmem],
        scratch_shapes=[
            pltpu.VMEM((n_tp, tok_dev, shard), bf16),
            pltpu.VMEM((tok_dev, model), bf16),
            pltpu.VMEM((tok_dev, 1), f32),
            pltpu.VMEM((6, model, width), bf16),
            pltpu.VMEM((n_tp, heads, block, 128), bf16),
            pltpu.VMEM((n_sp, n_tp, block, 128), bf16),
            pltpu.VMEM((tok_dev + 8, width), f32),
            pltpu.VMEM((8, width), f32),
            pltpu.VMEM((8, width), f32),
            pltpu.VMEM((tok_dev, width), bf16),
            pltpu.VMEM((n_tp, size, width), bf16),
            pltpu.VMEM((n_sp, n_tp, size, 128), bf16),
            pltpu.VMEM((n_tiles, size, 128), bf16),
            pltpu.VMEM((n_tiles + 1, HEAD_DIM, size), f32),
            pltpu.VMEM((n_tiles + 1, 8, size), f32),
            pltpu.VMEM((n_tp, size, size), bf16),
            pltpu.VMEM((n_tp, size, size), bf16),
            pltpu.VMEM((n_tp, 8, size), f32),
            pltpu.VMEM((n_tp, 8, size), f32),
            pltpu.VMEM((n_tiles, HEAD_DIM, size), bf16),
            pltpu.VMEM((n_tiles, 8, size), f32),
            pltpu.VMEM((heads * n_tp, HEAD_DIM, size), bf16),
            pltpu.VMEM((heads * n_tp, 8, size), f32),
            pltpu.VMEM(filter_readout.shape, bf16),
            pltpu.VMEM(attention_readout.shape, bf16),
            pltpu.VMEM((size, model), f32),
            pltpu.VMEM((size, n_tp * width), bf16),
            dma((8,)),
            dma((n_tp,)),
            dma((3, n_tp)),
            dma((3, n_tp)),
            dma((n_tp, heads)),
            dma((n_sp, n_tp)),
            dma((n_sp, n_tp)),
            dma((2,)),
            dma((n_tp,)),
            dma((n_tp,)),
            dma((n_tiles,)),
            dma((heads * n_tp,)),
            dma((n_tiles,)),
            dma((heads * n_tp,)),
        ],
        compiler_params=pltpu.CompilerParams(
            collective_id=0, has_side_effects=True, vmem_limit_bytes=60 * 1024 * 1024
        ),
        name="layer",
    )(
        tokens,
        norm_gain.reshape(1, model),
        signal_proj,
        postgate_proj,
        pregate_proj,
        query_proj,
        key_proj,
        value_proj,
        filter_taps,
        break_bias.T,
        filter_readout,
        attention_readout,
    )


def per_device_any(*operands):
    tok_dev = operands[0].shape[0]
    heads_dev = operands[9].shape[1]
    n_sp, n_tp = lax.axis_size("sp"), lax.axis_size("tp")
    fast = n_tp == 4 and n_sp == 2 * heads_dev and tok_dev == n_tp * 256 and operands[6].shape[1] == 256
    return (per_device_fast if fast else per_device)(*operands)


def solution(mesh):
    placed = (
        P("sp", "tp"),
        P(),
        P(None, "tp"),
        P(None, "tp"),
        P(None, "tp"),
        P(None, "tp"),
        P(None, "tp"),
        P(None, "tp"),
        P(None, "tp"),
        P("sp", "tp"),
        P(),
        P(),
    )
    return jax.shard_map(
        per_device_any,
        mesh=mesh,
        in_specs=placed,
        out_specs=(P(("sp", "tp"), None), P("tp", "sp")),
        check_vma=False,
    )
```

```python
import functools

import jax
import jax.numpy as jnp
from jax import lax
from jax.experimental import pallas as pl
from jax.experimental.pallas import tpu as pltpu
from jax.sharding import PartitionSpec as P

HEAD_DIM = 64
CONV_W = 3
KEY_CHUNK = 256


epsilon = 1e-06
mass_floor = 0.1
score_cap = 88.0
score_cap_fast = 43.0


def passed_along(block, axis, distance):
    devices = range(lax.axis_size(axis))
    route = [(i - distance, i) for i in devices if i - distance in devices]
    return lax.ppermute(block, axis, route)


def attention_kernel(tok_dev, share, rows, chain, part_ref, recv_ref, bias_ref, out_ref, acc, carry):
    chunk = KEY_CHUNK
    tile = pl.program_id(0)
    tiles_block = share // rows
    block = tile // tiles_block
    inner = (tile % tiles_block) * rows
    row_start = block * tok_dev + part_ref[0] * share + inner
    chunks_block = tok_dev // chunk
    acc[...] = jnp.zeros_like(acc)
    carry[...] = jnp.zeros_like(carry)
    later = lax.broadcasted_iota(jnp.int32, (chunk, chunk), 0)
    earlier = lax.broadcasted_iota(jnp.int32, (chunk, chunk), 1)
    after = jnp.where(later > earlier, 1.0, 0.0).astype(jnp.bfloat16)

    def step(masked, index):
        offset = pl.multiple_of((index % chunks_block) * chunk, chunk)
        key_value = recv_ref[index // chunks_block, pl.ds(offset, chunk), :]
        bias = bias_ref[index]
        for link in range(rows // chain):
            place = pl.ds(link * chain, chain)
            query_place = pl.multiple_of(tok_dev + inner + link * chain, chain)
            query = recv_ref[block, pl.ds(query_place, chain), :]
            scores = lax.dot_general(
                query, key_value, (((1,), (1,)), ((), ())), preferred_element_type=jnp.float32
            )
            scores = jnp.minimum(scores + bias, score_cap)
            lost = jnp.log(1.0 + jnp.exp(scores))
            own = scores - lost
            if masked:
                row_ids = lax.broadcasted_iota(jnp.int32, scores.shape, 0) + (row_start + link * chain)
                col_ids = lax.broadcasted_iota(jnp.int32, scores.shape, 1) + index * chunk
                allowed = col_ids < row_ids
                lost = jnp.where(allowed, lost, 0.0)
            behind = jnp.dot(lost.astype(jnp.bfloat16), after, preferred_element_type=jnp.float32)
            before = carry[place, :]
            weights = jnp.exp(own - (behind + before))
            if masked:
                weights = jnp.where(allowed, weights, 0.0)
            acc[place, :] += jnp.dot(
                weights.astype(jnp.bfloat16), key_value, preferred_element_type=jnp.float32
            )
            carry[place, :] = before + (behind[:, :1] + lost[:, :1])

    full = row_start // chunk
    top = (row_start + rows + chunk - 1) // chunk

    @pl.loop(0, top - full)
    def _(i):
        step(True, top - 1 - i)

    @pl.loop(0, full)
    def _(i):
        step(False, full - 1 - i)

    remain = jnp.broadcast_to(-carry[...], acc.shape)
    high = remain.astype(jnp.bfloat16)
    rest = remain - high.astype(jnp.float32)
    middle = rest.astype(jnp.bfloat16)
    low = (rest - middle.astype(jnp.float32)).astype(jnp.bfloat16)
    lane = lax.broadcasted_iota(jnp.int32, acc.shape, 1)
    packed = jnp.where(lane == 0, high.astype(jnp.float32), 0.0)
    packed = jnp.where(lane == 1, middle.astype(jnp.float32), packed)
    packed = jnp.where(lane == 2, low.astype(jnp.float32), packed)
    out_ref[0] = jnp.where(lane >= HEAD_DIM, acc[...], packed).astype(jnp.bfloat16)


def attend(received, bias_row, part, tok_dev):
    n_sp, _, lanes = received.shape
    share = received.shape[1] - tok_dev
    rows = min(512, share)
    chain = min(256, rows)
    tiles_block = share // rows
    bias3 = bias_row.reshape(n_sp * tok_dev // KEY_CHUNK, 1, KEY_CHUNK)
    pairs = n_sp * share * n_sp * tok_dev // 2
    return pl.pallas_call(
        functools.partial(attention_kernel, tok_dev, share, rows, chain),
        out_shape=jax.ShapeDtypeStruct((n_sp, share, lanes), jnp.bfloat16),
        grid_spec=pltpu.PrefetchScalarGridSpec(
            num_scalar_prefetch=1,
            grid=(n_sp * tiles_block,),
            in_specs=[
                pl.BlockSpec(received.shape, lambda i, part: (0, 0, 0)),
                pl.BlockSpec(bias3.shape, lambda i, part: (0, 0, 0)),
            ],
            out_specs=pl.BlockSpec((1, rows, lanes), lambda i, part: (i // tiles_block, i % tiles_block, 0)),
            scratch_shapes=[
                pltpu.VMEM((rows, lanes), jnp.float32),
                pltpu.VMEM((rows, 1), jnp.float32),
            ],
        ),
        compiler_params=pltpu.CompilerParams(
            dimension_semantics=("arbitrary",), vmem_limit_bytes=32 * 1024 * 1024
        ),
        cost_estimate=pl.CostEstimate(
            flops=pairs * (4 * lanes + 2 * KEY_CHUNK), bytes_accessed=received.size * 2, transcendentals=3 * pairs
        ),
    )(part, received, bias3)


def per_device(
    tokens,
    norm_gain,
    signal_proj,
    postgate_proj,
    pregate_proj,
    query_proj,
    key_proj,
    value_proj,
    filter_taps,
    break_bias,
    filter_readout,
    attention_readout,
):
    tok_dev = tokens.shape[0]
    heads_dev = break_bias.shape[1]
    n_sp = lax.axis_size("sp")
    parts = n_sp // heads_dev
    share = tok_dev // parts
    position = lax.axis_index("sp")
    all_bias = lax.all_gather(break_bias.T, "sp", axis=1, tiled=True)
    all_bias, tokens = lax.optimization_barrier((all_bias, tokens))
    bias_row = lax.dynamic_slice_in_dim(all_bias, position // parts, 1, 0).astype(jnp.float32)
    model = key_proj.shape[0]
    key_value_proj = jnp.concatenate(
        [
            key_proj.reshape(model, heads_dev, HEAD_DIM),
            value_proj.reshape(model, heads_dev, HEAD_DIM),
        ],
        axis=2,
    ).reshape(model, 2 * heads_dev * HEAD_DIM)
    whole_rows = lax.all_gather(tokens, "tp", axis=1, tiled=True)
    widened = whole_rows.astype(jnp.float32)
    inverse = lax.rsqrt(jnp.mean(widened * widened, axis=1) + epsilon)
    scaled = (widened * norm_gain[None, :]).astype(jnp.bfloat16)

    def project(weight, factor=1.0):
        product = jnp.dot(scaled, weight, preferred_element_type=jnp.float32)
        return (product * inverse[:, None]).astype(jnp.bfloat16) * jnp.bfloat16(factor)

    key_values = project(key_value_proj).reshape(tok_dev, heads_dev, 2 * HEAD_DIM)
    queries = project(query_proj, HEAD_DIM ** (-0.5)).reshape(tok_dev, heads_dev, HEAD_DIM)
    queries = jnp.pad(queries, ((0, 0), (0, 0), (0, HEAD_DIM)))
    key_values = key_values.transpose(1, 0, 2)
    queries = queries.transpose(1, 0, 2)
    outgoing = jnp.stack(
        [
            jnp.concatenate([key_values, queries[:, part * share : (part + 1) * share]], axis=1)
            for part in range(parts)
        ],
        axis=1,
    ).reshape(n_sp, tok_dev + share, 2 * HEAD_DIM)
    received = lax.all_to_all(outgoing, "sp", split_axis=0, concat_axis=0, tiled=True)
    signal, post_gate, pre_gate = (project(w) for w in (signal_proj, postgate_proj, pregate_proj))
    rim_width = CONV_W - 1
    rim_signal, rim_pre = passed_along(
        (signal[tok_dev - rim_width :], pre_gate[tok_dev - rim_width :]), "sp", 1
    )
    extended = jnp.concatenate(
        [
            rim_pre.astype(jnp.float32) * rim_signal.astype(jnp.float32),
            pre_gate.astype(jnp.float32) * signal.astype(jnp.float32),
        ],
        axis=0,
    )
    tap_values = filter_taps.astype(jnp.float32)
    running = jnp.zeros((tok_dev, extended.shape[1]), jnp.float32)
    for offset in range(CONV_W):
        running = running + tap_values[offset][None, :] * extended[offset : offset + tok_dev]
    filtered = (post_gate.astype(jnp.float32) * running).astype(jnp.bfloat16)
    filter_rows = lax.all_to_all(filtered, "tp", split_axis=0, concat_axis=1, tiled=True)

    part = (position % parts).astype(jnp.int32).reshape(1)
    computed = attend(received, bias_row, part, tok_dev)
    returned = lax.all_to_all(computed, "sp", split_axis=0, concat_axis=0, tiled=True)
    returned = returned.reshape(heads_dev, tok_dev, 2 * HEAD_DIM)
    attended = returned[:, :, HEAD_DIM:].transpose(1, 0, 2).reshape(tok_dev, heads_dev * HEAD_DIM)
    remain = jnp.sum(returned[:, :, :3].astype(jnp.float32), axis=2)
    mass_logarithm = jnp.log(jnp.maximum(-jnp.expm1(remain), mass_floor))
    attended_rows = lax.all_to_all(attended, "tp", split_axis=0, concat_axis=1, tiled=True)
    mixed = (
        jnp.dot(filter_rows, filter_readout, preferred_element_type=jnp.float32)
        + jnp.dot(attended_rows, attention_readout, preferred_element_type=jnp.float32)
    ).astype(jnp.bfloat16)
    return (mixed, mass_logarithm)


def tile_core(u):
    return jnp.where((u == 0) | (u == 3), 0, 1)


def tile_at(index, core):
    return (index // 2) * 4 + jnp.where(index % 2 == 0, core, 3 - core)


def scatter_matrix(rows_are_places, n):
    row = lax.broadcasted_iota(jnp.int32, (n, n), 0)
    col = lax.broadcasted_iota(jnp.int32, (n, n), 1)
    place, slot = (row, col) if rows_are_places else (col, row)
    span = n // 8
    hit = place == (slot % 8) * span + (span - 1 - slot // 8)
    return jnp.where(hit, 1.0, 0.0).astype(jnp.bfloat16)


def remote(src, dst, send, recv, sp, tp):
    return pltpu.make_async_remote_copy(
        src_ref=src,
        dst_ref=dst,
        send_sem=send,
        recv_sem=recv,
        device_id={"sp": sp, "tp": tp},
        device_id_type=pl.DeviceIdType.MESH,
    )


def meet(peers):
    barrier = pltpu.get_barrier_semaphore()
    for sp, tp in peers:
        pl.semaphore_signal(
            barrier, inc=1, device_id={"sp": sp, "tp": tp}, device_id_type=pl.DeviceIdType.MESH
        )
    pl.semaphore_wait(barrier, len(peers))


def later_product(total):
    n = total.shape[0]
    row = lax.broadcasted_iota(jnp.int32, total.shape, 0)
    x = jnp.where(row < n - 1, pltpu.roll(total, n - 1, 0), 1.0)
    k = 1
    while k < n:
        x = x * jnp.where(row < n - k, pltpu.roll(x, n - k, 0), 1.0)
        k *= 2
    return x


def layer_kernel(
    n_sp,
    heads,
    tokens,
    gain,
    signal_w,
    post_w,
    pre_w,
    query_w,
    key_w,
    value_w,
    taps,
    bias,
    filter_w,
    attend_w,
    mixed,
    logs,
    xbuf,
    scaled,
    squares,
    weights,
    outgoing,
    gathered,
    product,
    rim,
    rim_out,
    ready,
    filt,
    keys,
    quer,
    acc,
    carry,
    w0,
    w1,
    r0,
    r1,
    s0,
    s1,
    tiles,
    mass,
    arrived,
    marks,
    wf,
    wa,
    partial,
    attended,
    w_sem,
    own_sem,
    ag_send,
    ag_recv,
    kv_send,
    kv_recv,
    fwd_send,
    rim_sem,
    filt_send,
    filt_recv,
    a_send,
    a_recv,
    m_send,
    m_recv,
):
    p = lax.axis_index("sp")
    t = lax.axis_index("tp")
    y, c = t // 2, t % 2
    mate = 2 * y + 1 - c
    cross = 2 * (1 - y) + c
    tok_dev, shard = tokens.shape
    n_tp = xbuf.shape[0]
    size = tok_dev // n_tp
    width = key_w.shape[1]
    model = n_tp * shard
    half_sp = n_sp // 2
    upper = p // half_sp
    primary = c == p // heads
    owner = 2 * y + p // heads
    head = owner * heads + p % heads
    total_heads = arrived.shape[0]
    n_tiles = tiles.shape[0]
    groups = size // 8

    sources = (key_w, query_w, value_w, signal_w, pre_w, post_w)
    loads = [pltpu.make_async_copy(w, weights.at[i], w_sem.at[i]) for i, w in enumerate(sources)]
    loads.append(pltpu.make_async_copy(filter_w, wf, w_sem.at[6]))
    loads.append(pltpu.make_async_copy(attend_w, wa, w_sem.at[7]))
    own = [
        pltpu.make_async_copy(
            tokens.at[pl.ds(i * size, size)], xbuf.at[t, pl.ds(i * size, size)], own_sem.at[i]
        )
        for i in range(n_tp)
    ]
    own[0].start()
    for load in loads[:3]:
        load.start()
    peers = []
    for a in range(n_sp):
        for b in range(n_tp):
            if a or b:
                peers.append(((p + a) % n_sp, (t + b) % n_tp))
    meet(peers)

    def token_copy(kind, i):
        rows = pl.ds(i * size, size)
        if kind == 0:
            return remote(tokens.at[rows], xbuf.at[t, rows], ag_send.at[0, i], ag_recv.at[0, i], p, cross)
        if kind == 1:
            return remote(tokens.at[rows], xbuf.at[t, rows], ag_send.at[1, i], ag_recv.at[1, i], p, mate)
        return remote(
            xbuf.at[cross, rows], xbuf.at[cross, rows], ag_send.at[2, i], ag_recv.at[2, i], p, mate
        )

    for i in range(n_tp):
        token_copy(0, i).start()
    for i in range(n_tp):
        token_copy(1, i).start()
    for copy in own[1:]:
        copy.start()
    for load in loads[3:]:
        load.start()
    for load in loads[:6]:
        load.wait()
    order = scatter_matrix(False, size)
    back = scatter_matrix(True, size)
    lane = lax.broadcasted_iota(jnp.int32, (size, 128), 1)
    step = 32

    def kv_copy(i, h):
        target = c * heads + h
        stays = target == p
        sp = jnp.where(stays, p, target)
        tp = jnp.where(stays, mate, t)
        return remote(
            outgoing.at[i, h], gathered.at[p, i], kv_send.at[i, h], kv_recv.at[p, i], sp, tp
        )

    row16 = lax.broadcasted_iota(jnp.int32, (16, 128), 0)
    lane16 = lax.broadcasted_iota(jnp.int32, (16, 128), 1)
    units = [
        jnp.where((row16 == k) & (lane16 == HEAD_DIM), 1.0, 0.0).astype(jnp.bfloat16) for k in range(2)
    ]
    constant = jnp.where(lane == HEAD_DIM, 1.0, 0.0)

    def arrival(b, i):
        return remote(outgoing.at[i, 0], gathered.at[b, i], fwd_send.at[b, i], kv_recv.at[b, i], p, mate)

    def forward(b, i):
        return remote(gathered.at[b, i], gathered.at[b, i], fwd_send.at[b, i], kv_recv.at[b, i], p, mate)

    def accept(base, i):
        @pl.loop(0, half_sp)
        def _(k):
            b = base + k

            @pl.when(jnp.logical_not(primary & (b == p)))
            def _():
                arrival(b, i).wait_recv()

            @pl.when(primary & (b != p))
            def _():
                forward(b, i).start()

        for k in range(half_sp):
            b = base + k
            kq = gathered[b, i, 0:size, :].astype(jnp.float32)
            tail = gathered[b, i, size + 2 * HEAD_DIM :, :]
            column = jnp.concatenate(
                [
                    lax.dot_general(tail, unit, (((0,), (0,)), ((), ())), preferred_element_type=jnp.float32)
                    for unit in units
                ],
                axis=0,
            )
            keys[b, i] = jnp.where(lane < HEAD_DIM, kq, column).astype(jnp.bfloat16)

        @pl.when(tile_core(i) == c)
        def _():
            for k in range(half_sp):
                b = base + k
                index = b * (n_tp // 2) + i // 2
                rolled = pltpu.roll(gathered[b, i, 0:size, :].astype(jnp.float32), HEAD_DIM, 1)
                quer[index] = jnp.where(lane < HEAD_DIM, rolled, constant).astype(jnp.bfloat16)

    tap_values = taps[...].astype(jnp.float32)
    rim_copy = remote(rim_out, rim, rim_sem.at[0], rim_sem.at[1], (p + 1) % n_sp, t)

    def gate(i, x, inv):
        outs = []
        for index in range(3, 6):
            y_ = jnp.dot(x, weights[index], preferred_element_type=jnp.float32)
            outs.append((y_ * inv).astype(jnp.bfloat16))
        at = pl.ds(pl.multiple_of(8 + i * size, 8), size)
        product[at, :] = outs[1].astype(jnp.float32) * outs[0].astype(jnp.float32)
        ready[pl.ds(pl.multiple_of(i * size, size), size), :] = outs[2]

    def convolve(i):
        around = product[pl.ds(pl.multiple_of(i * size, size), size + 8), :]
        running = jnp.zeros((size, width), jnp.float32)
        for w in range(CONV_W):
            start = 8 - (CONV_W - 1) + w
            running = running + tap_values[w : w + 1, :] * around[start : start + size, :]
        rows = pl.ds(pl.multiple_of(i * size, size), size)
        done = (ready[rows, :].astype(jnp.float32) * running).astype(jnp.bfloat16)
        ready[rows, :] = done

        @pl.when(t == i)
        def _():
            filt[i] = done

    def filt_copy(u):
        return remote(ready.at[pl.ds(u * size, size)], filt.at[t], filt_send.at[u], filt_recv.at[t], p, u)

    @pl.loop(0, n_tp)
    def _(i):
        rows = pl.ds(pl.multiple_of(i * size, size), size)
        pltpu.make_async_copy(tokens.at[rows], xbuf.at[t, rows], own_sem.at[i]).wait()
        token_copy(0, i).wait_recv()
        token_copy(2, i).start()
        token_copy(1, i).wait_recv()
        token_copy(2, i).wait_recv()

        @pl.loop(0, size // step)
        def _(k0):
            place = pl.ds(pl.multiple_of(i * size + k0 * step, step), step)
            total = jnp.zeros((step, 128), jnp.float32)
            for part in range(n_tp):
                x = xbuf[part, place, :].astype(jnp.float32)
                square = x * x
                for k in range(0, shard, 128):
                    total = total + square[:, k : k + 128]
                columns = slice(part * shard, (part + 1) * shard)
                scaled[place, columns] = (x * gain[:, columns]).astype(jnp.bfloat16)
            squares[pl.ds(pl.multiple_of(k0 * step, step), step), :] = total

        x = scaled[rows, :]
        total = jnp.sum(squares[...], axis=1, keepdims=True)
        inv = lax.rsqrt(total * (1.0 / model) + epsilon)

        def project(index):
            y_ = jnp.dot(x, weights[index], preferred_element_type=jnp.float32)
            return (y_ * inv).astype(jnp.bfloat16)

        k_rows = jnp.dot(order, project(0), preferred_element_type=jnp.float32)
        q_rows = jnp.dot(order, project(1), preferred_element_type=jnp.float32) * (HEAD_DIM**-0.5)
        v_cols = jnp.dot(order, project(2), preferred_element_type=jnp.float32).T
        bias_rows = jnp.dot(bias[:, rows], back, preferred_element_type=jnp.float32)
        pair_width = 2 * HEAD_DIM
        for h in range(heads):
            pair = slice((h // 2) * pair_width, (h // 2 + 1) * pair_width)
            kp, qp = k_rows[:, pair], q_rows[:, pair]
            if h % 2 == 0:
                kq = jnp.where(lane < HEAD_DIM, kp, pltpu.roll(qp, HEAD_DIM, 1))
            else:
                kq = jnp.where(lane < HEAD_DIM, pltpu.roll(kp, HEAD_DIM, 1), qp)
            kq = kq.astype(jnp.bfloat16)
            vb = v_cols[h * HEAD_DIM : (h + 1) * HEAD_DIM, :].astype(jnp.bfloat16)
            row = lax.broadcasted_iota(jnp.int32, (16, 128), 0)
            tail = jnp.where(row == 0, bias_rows[h : h + 1, :128], 0.0)
            tail = jnp.where(row == 1, bias_rows[h : h + 1, 128:], tail).astype(jnp.bfloat16)

            def put(ref):
                ref[0:size, :] = kq
                ref[size : size + HEAD_DIM, :] = vb[:, :128]
                ref[size + HEAD_DIM : size + 2 * HEAD_DIM, :] = vb[:, 128:]
                ref[size + 2 * HEAD_DIM :, :] = tail

            put(outgoing.at[i, h])

            @pl.when(c * heads + h == p)
            def _():
                put(gathered.at[p, i])

            kv_copy(i, h).start()

        gate(i, x, inv)

        @pl.when(i == n_tp - 1)
        def _():
            rim_out[...] = product[tok_dev : tok_dev + 8, :]
            rim_copy.start()

        @pl.when(i > 0)
        def _():
            convolve(i)

        @pl.when(i >= 2)
        def _():
            accept(upper * half_sp, i - 2)

    for u in range(1, n_tp):

        @pl.when(t != u)
        def _():
            filt_copy(u).start()

    @pl.loop(n_tp - 2, n_tp)
    def _(i):
        accept(upper * half_sp, i)

    rim_copy.wait()
    product[0:8, :] = jnp.where(p > 0, rim[...], 0.0)
    convolve(0)

    @pl.when(t != 0)
    def _():
        filt_copy(0).start()

    col = lax.broadcasted_iota(jnp.int32, (8, size), 1)
    place8 = (col % 8) * groups + (groups - 1) - col // 8
    relative = place8 - lax.broadcasted_iota(jnp.int32, (8, size), 0) * groups
    wb, rb, sb = (w0, w1), (r0, r1), (s0, s1)

    def score(index, b, s):
        return lax.dot_general(
            keys[b, s], quer[index], (((1,), (1,)), ((), ())), preferred_element_type=jnp.float32
        )

    def early(slot, index, b, masked):
        tile = tile_at(index, c)
        for s in range(n_tp):
            scores = score(index, b, s) if s else sb[1 - slot]
            shift = (tile % n_tp - s) * size
            run = None
            for j in range(groups):
                e = jnp.exp(jnp.minimum(scores[8 * j : 8 * j + 8, :], score_cap_fast))
                if masked:
                    e = jnp.where(relative + shift > groups - 1 - j, e, 0.0)
                r = 1.0 / (1.0 + e)
                run = r if run is None else run * r
                w = e * run
                if j % 2:
                    pair = jnp.concatenate([before, w], axis=0).astype(jnp.bfloat16)
                    wb[slot][s, 8 * (j - 1) : 8 * (j + 1), :] = pair
                before = w
            rb[slot][s] = run

    def late(slot, index, b):
        first = b == tile_at(index, c) // n_tp
        running = jnp.where(first, 1.0, carry[index])
        total = jnp.where(first, 0.0, acc[index])
        for s in range(n_tp - 1, -1, -1):
            run = rb[slot][s]
            factor = later_product(run) * running
            running = jnp.broadcast_to((factor * run)[:1], run.shape)
            twice = jnp.concatenate([factor, factor], axis=0).astype(jnp.bfloat16)
            pieces = [wb[slot][s, 16 * j : 16 * j + 16, :] * twice for j in range(groups // 2)]
            values = jnp.concatenate(
                [
                    gathered[b, s, size : size + HEAD_DIM, :],
                    gathered[b, s, size + HEAD_DIM : size + 2 * HEAD_DIM, :],
                ],
                axis=1,
            )
            total = total + jnp.dot(
                values, jnp.concatenate(pieces, axis=0), preferred_element_type=jnp.float32
            )
        acc[index] = total
        carry[index] = running

    def tile_copy(index):
        tile = tile_at(index, c)
        b, u = tile // n_tp, tile % n_tp
        return remote(tiles.at[index], arrived.at[head], a_send.at[index], a_recv.at[head], b, u)

    def mark_copy(index):
        tile = tile_at(index, c)
        b, u = tile // n_tp, tile % n_tp
        slot = p % heads * n_tp + u
        return remote(mass.at[index], marks.at[slot], m_send.at[index], m_recv.at[slot], b, owner)

    def ownership(index):
        tile = tile_at(index, c)
        b, u = tile // n_tp, tile % n_tp
        return u, (b == p) & (u == t), (b == p) & (owner == t)

    def hand_over(index):
        u, own_tile, own_mark = ownership(index)
        value = acc[index].astype(jnp.bfloat16)
        mark = jnp.log(jnp.maximum(1.0 - carry[index], mass_floor))
        tiles[index] = value
        mass[index] = mark

        @pl.when(own_tile)
        def _():
            arrived[head] = value

        @pl.when(jnp.logical_not(own_tile))
        def _():
            tile_copy(index).start()

        @pl.when(own_mark)
        def _():
            marks[p % heads * n_tp + u] = mark

        @pl.when(jnp.logical_not(own_mark))
        def _():
            mark_copy(index).start()

    half_tiles = n_tiles // 2
    per_block = n_tp // 2

    def block_of(index):
        return tile_at(index, c) // n_tp

    def sweep(base, from_diagonal, low, items, sends):
        steps = items + 1
        skip = steps % 2
        spare = jnp.int32(n_tiles)

        def start_of(index):
            return jnp.where(from_diagonal, block_of(index), half_sp - 1)

        def half(z, m, state):
            i1, b1, i2, b2 = state
            last = b1 == low
            after = jnp.minimum(i1 + 1, base + half_tiles - 1)
            advance = m >= 0
            ni = jnp.where(advance & last, after, i1)
            nb = jnp.where(advance, jnp.where(last, start_of(after), b1 - 1), b1)

            def go(masked):
                late(z, i2, b2)
                early(1 - z, i1, b1, masked)
                sb[1 - z][...] = score(ni, nb, 0)

            lax.cond(b1 == block_of(i1), lambda: go(True), lambda: go(False))

            @pl.when(sends & (b2 == 0) & (m >= 1))
            def _():
                hand_over(i2)

            return ni, nb, jnp.where(advance, i1, spare), b1

        def body(k, state):
            for z in range(2):
                state = half(z, 2 * k + z - skip, state)
            return state

        first = start_of(base)
        rounds = jnp.where(items > 0, (steps + skip) // 2, 0)
        sb[0][...] = score(base, first, 0)
        lax.fori_loop(0, rounds, body, (base, first, spare, first))

    triangle = per_block * (half_sp * (half_sp + 1) // 2)
    square = per_block * half_sp * half_sp
    is_upper = upper == 1

    @pl.loop(0, 3)
    def _(phase):
        near = phase == 0

        @pl.when(phase == 1)
        def _():
            loads[6].wait()
            for k in range(1, n_tp):
                u = (t + k) % n_tp
                remote(ready.at[pl.ds(0, size)], filt.at[u], filt_send.at[u], filt_recv.at[u], p, u).wait()

            @pl.loop(0, model // 256)
            def _(k):
                at = pl.ds(pl.multiple_of(k * 256, 256), 256)
                total = jnp.zeros((size, 256), jnp.float32)
                for part in range(n_tp):
                    total = total + jnp.dot(
                        filt[part],
                        wf[part * width : (part + 1) * width, at],
                        preferred_element_type=jnp.float32,
                    )
                partial[:, at] = total

            @pl.loop(0, n_tp)
            def _(i):
                accept((1 - upper) * half_sp, i)


        first_items = jnp.where(is_upper, square, triangle + square)
        last_items = jnp.where(is_upper, triangle, 0)
        sweep(
            jnp.where(near, upper * half_tiles, jnp.where(phase == 1, half_tiles, 0)),
            jnp.logical_not(is_upper & (phase == 1)),
            jnp.where(near, upper * half_sp, 0),
            jnp.where(near, triangle, jnp.where(phase == 1, first_items, last_items)),
            jnp.logical_not(near & is_upper),
        )

    loads[7].wait()
    mine = tile_core(t) == c

    @pl.loop(0, total_heads)
    def _(k):
        @pl.when(jnp.logical_not((k == head) & mine))
        def _():
            remote(tiles.at[0], arrived.at[k], a_send.at[0], a_recv.at[k], p, t).wait_recv()

    for part in range(n_tp):
        stack = jnp.concatenate([arrived[part * heads + h] for h in range(heads)], axis=0)
        rows = lax.dot_general(back, stack, (((1,), (1,)), ((), ())), preferred_element_type=jnp.float32)
        attended[:, part * width : (part + 1) * width] = rows.astype(jnp.bfloat16)

    @pl.loop(0, model // 256)
    def _(k):
        at = pl.ds(pl.multiple_of(k * 256, 256), 256)
        total = partial[:, at] + jnp.dot(attended[...], wa[:, at], preferred_element_type=jnp.float32)
        mixed[:, at] = total.astype(jnp.bfloat16)

    @pl.loop(0, heads)
    def _(h):
        for u in range(n_tp):
            own_mark = (p == c * heads + h) & (tile_core(u) == c)

            @pl.when(jnp.logical_not(own_mark))
            def _():
                slot = h * n_tp + u
                remote(mass.at[0], marks.at[slot], m_send.at[0], m_recv.at[slot], p, t).wait_recv()

    for u in range(n_tp):
        row = lax.broadcasted_iota(jnp.int32, (8, size), 0)
        value = jnp.zeros((8, size), jnp.float32)
        for h in range(heads):
            value = jnp.where(row == h, marks[h * n_tp + u], value)
        total = jnp.zeros((8, size), jnp.float32)
        for _ in range(3):
            high = value.astype(jnp.bfloat16)
            value = value - high.astype(jnp.float32)
            total = total + jnp.dot(high, order, preferred_element_type=jnp.float32)
        logs[:, u * size : (u + 1) * size] = total[:heads]

    @pl.loop(0, n_tiles)
    def _(index):
        u, own_tile, own_mark = ownership(index)

        @pl.when(jnp.logical_not(own_tile))
        def _():
            tile_copy(index).wait_send()

        @pl.when(jnp.logical_not(own_mark))
        def _():
            mark_copy(index).wait_send()

    @pl.when(primary)
    def _():
        @pl.loop(0, n_tp)
        def _(i):
            @pl.loop(1, n_sp)
            def _(k):
                forward((p + k) % n_sp, i).wait_send()

    for i in range(n_tp):
        for kind in range(3):
            token_copy(kind, i).wait_send()
        for h in range(heads):
            kv_copy(i, h).wait_send()


def per_device_fast(
    tokens,
    norm_gain,
    signal_proj,
    postgate_proj,
    pregate_proj,
    query_proj,
    key_proj,
    value_proj,
    filter_taps,
    break_bias,
    filter_readout,
    attention_readout,
):
    n_sp, n_tp = lax.axis_size("sp"), lax.axis_size("tp")
    tok_dev, shard = tokens.shape
    heads = break_bias.shape[1]
    width = key_proj.shape[1]
    model = n_tp * shard
    size = tok_dev // n_tp
    block = size + 2 * HEAD_DIM + 16
    n_tiles = n_sp * n_tp // 2
    vmem = pl.BlockSpec(memory_space=pltpu.VMEM)
    anywhere = pl.BlockSpec(memory_space=pl.ANY)
    dma = pltpu.SemaphoreType.DMA
    bf16, f32 = jnp.bfloat16, jnp.float32
    return pl.pallas_call(
        functools.partial(layer_kernel, n_sp, heads),
        out_shape=[
            jax.ShapeDtypeStruct((size, model), bf16),
            jax.ShapeDtypeStruct((heads, tok_dev), f32),
        ],
        in_specs=[anywhere, vmem] + [anywhere] * 6 + [vmem, vmem, anywhere, anywhere],
        out_specs=[vmem, vmem],
        scratch_shapes=[
            pltpu.VMEM((n_tp, tok_dev, shard), bf16),
            pltpu.VMEM((tok_dev, model), bf16),
            pltpu.VMEM((size, 128), f32),
            pltpu.VMEM((6, model, width), bf16),
            pltpu.VMEM((n_tp, heads, block, 128), bf16),
            pltpu.VMEM((n_sp, n_tp, block, 128), bf16),
            pltpu.VMEM((tok_dev + 8, width), f32),
            pltpu.VMEM((8, width), f32),
            pltpu.VMEM((8, width), f32),
            pltpu.VMEM((tok_dev, width), bf16),
            pltpu.VMEM((n_tp, size, width), bf16),
            pltpu.VMEM((n_sp, n_tp, size, 128), bf16),
            pltpu.VMEM((n_tiles, size, 128), bf16),
            pltpu.VMEM((n_tiles + 1, HEAD_DIM, size), f32),
            pltpu.VMEM((n_tiles + 1, 8, size), f32),
            pltpu.VMEM((n_tp, size, size), bf16),
            pltpu.VMEM((n_tp, size, size), bf16),
            pltpu.VMEM((n_tp, 8, size), f32),
            pltpu.VMEM((n_tp, 8, size), f32),
            pltpu.VMEM((size, size), f32),
            pltpu.VMEM((size, size), f32),
            pltpu.VMEM((n_tiles, HEAD_DIM, size), bf16),
            pltpu.VMEM((n_tiles, 8, size), f32),
            pltpu.VMEM((heads * n_tp, HEAD_DIM, size), bf16),
            pltpu.VMEM((heads * n_tp, 8, size), f32),
            pltpu.VMEM(filter_readout.shape, bf16),
            pltpu.VMEM(attention_readout.shape, bf16),
            pltpu.VMEM((size, model), f32),
            pltpu.VMEM((size, n_tp * width), bf16),
            dma((8,)),
            dma((n_tp,)),
            dma((3, n_tp)),
            dma((3, n_tp)),
            dma((n_tp, heads)),
            dma((n_sp, n_tp)),
            dma((n_sp, n_tp)),
            dma((2,)),
            dma((n_tp,)),
            dma((n_tp,)),
            dma((n_tiles,)),
            dma((heads * n_tp,)),
            dma((n_tiles,)),
            dma((heads * n_tp,)),
        ],
        compiler_params=pltpu.CompilerParams(
            collective_id=0, has_side_effects=True, vmem_limit_bytes=60 * 1024 * 1024
        ),
        name="layer",
    )(
        tokens,
        norm_gain.reshape(1, model),
        signal_proj,
        postgate_proj,
        pregate_proj,
        query_proj,
        key_proj,
        value_proj,
        filter_taps,
        break_bias.T,
        filter_readout,
        attention_readout,
    )


def per_device_any(*operands):
    tok_dev = operands[0].shape[0]
    heads_dev = operands[9].shape[1]
    n_sp, n_tp = lax.axis_size("sp"), lax.axis_size("tp")
    fast = n_tp == 4 and n_sp == 2 * heads_dev and tok_dev == n_tp * 256 and operands[6].shape[1] == 256
    return (per_device_fast if fast else per_device)(*operands)


def solution(mesh):
    placed = (
        P("sp", "tp"),
        P(),
        P(None, "tp"),
        P(None, "tp"),
        P(None, "tp"),
        P(None, "tp"),
        P(None, "tp"),
        P(None, "tp"),
        P(None, "tp"),
        P("sp", "tp"),
        P(),
        P(),
    )
    return jax.shard_map(
        per_device_any,
        mesh=mesh,
        in_specs=placed,
        out_specs=(P(("sp", "tp"), None), P("tp", "sp")),
        check_vma=False,
    )
```
